768 devices in a mesh: ep: 24 (over z, core), tp: 32 (over y, x).
Axes of the slice: x: 4, y: 8, z: 12, core: 2. Of those that a mesh axis runs over, the one named last changes fastest.
Arguments:
- hidden: bfloat16 [384, 4096], P('ep', 'tp'), may hold values from -6 to 6
- norm_gain: float32 [4096], replicated, may hold values from 0.1 to 1.9
- routes: int32 [384, 4], P('ep'), may hold values from 0 to 47, all different within a row; in each aligned block of 16 rows (0 to 15, 16 to 31, ...) at most 3 rows name the same one
- route_weights: float32 [384, 4], P('ep'), may hold values from 0.1 to 1
- gate_weight: bfloat16 [48, 1024, 4096], P('ep', 'tp'), may hold values from -0.09375 to 0.09375
- up_weight: bfloat16 [48, 1024, 4096], P('ep', 'tp'), may hold values from -0.09375 to 0.09375
- down_weight: bfloat16 [48, 1024, 4096], P('ep', 'tp'), may hold values from -0.375 to 0.375
- shared_gate: bfloat16 [1024, 4096], P('tp'), may hold values from -0.09375 to 0.09375
- shared_up: bfloat16 [1024, 4096], P('tp'), may hold values from -0.09375 to 0.09375
- shared_down: bfloat16 [1024, 4096], P('tp'), may hold values from -0.375 to 0.375
Outputs:
- mixed: bfloat16 [384, 4096], P('ep', 'tp')
The draws below stay inside these ranges and needn't reach their ends.
Inputs may be any that keep to these rules, and one draw needn't show every extreme that they name: `routes`: each row names 4 different experts; among the rows of one index of ep (aligned blocks of 16 rows) no expert is named more than 3 times, a bound that some block reaches.
All inputs are finite; a program needn't handle non-finite values.
Results may differ from the reference program's by a relative error of at most 0.017.
Values may be sent and summed in bfloat16 or wider, within the bound.
No kernel may reach another device: no remote copies, remote signals or barrier semaphores. Data moves between devices by JAX's collectives and lax.ppermute only.
A program may use at most 64 MiB of HBM per device.

```python
import math
import jax
import jax.numpy as jnp
import numpy as np
from jax import lax

D = 4096
FF = 1024
FFS = 1024
TOP_K = 4
TOK_DEV = 16
EXPERTS = 48
CAP = 3
TOKENS = 384
N_EP = 24
N_TP = 32


def with_spikes(values, rng, source, target, blocks, factor):
    owner, partner = [(jnp.arange(values.shape[dim]) // (values.shape[dim] // blocks)).reshape([-1 if axis == dim else 1 for axis in range(values.ndim)]) for dim in (source, target)]
    chosen = jax.random.permutation(rng, blocks)[partner]
    strong = (owner == chosen) | (owner == (partner + blocks // 2) % blocks)
    return jnp.where(strong, factor * values, values)


def levels(own_key, extent, shards, smallest, largest):
    def one(axis_at, shards_of):
        heights = jax.random.uniform(jax.random.fold_in(jax.random.fold_in(own_key, 6), axis_at), (shards_of,), jnp.float32, smallest / len(shards), largest / len(shards))
        return jnp.repeat(jnp.exp(heights), extent[axis_at] // shards_of).reshape((-1,) + (1,) * (len(extent) - axis_at - 1))

    gain = one(*shards[0])
    for cut in shards[1:]:
        gain = gain * one(*cut)
    return gain


def shared_out(stream_key, own, number, rows, number_of, top, limit, lean):
    order = jax.random.permutation(stream_key, number_of)
    crowded, ordinary = shares(number_of, rows * top, limit, lean, True), shares(number_of, rows * top, limit, lean, False)
    places = jnp.arange(number_of)

    def named(sizes, rotation):
        used = int((sizes > 0).sum())
        fixed = max(1, used // 4)
        shifted = fixed + (places - fixed + rotation * (used - fixed)) % max(1, number_of - fixed)
        return jnp.zeros((number_of,), jnp.int32).at[order[jnp.where(places < fixed, places, shifted)]].set(jnp.asarray(sizes, jnp.int32))

    sizes = jnp.where(number % 4 == 0, named(crowded, number // 4), named(ordinary, number - number // 4 - 1))
    mixed = jax.random.permutation(jax.random.fold_in(own, 3), number_of)
    source_of, taker = mixed[0:number_of // 2 * 2:2], mixed[1:number_of // 2 * 2:2]
    margin = jnp.minimum(sizes[source_of] - 1, limit - sizes[taker]) // 2
    margin = jnp.where((source_of == order[0]) | (taker == order[0]) | (sizes[taker] == 0), 0, jnp.maximum(margin, 0))
    shifted = jax.random.randint(jax.random.fold_in(own, 4), (number_of // 2,), 0, 1 << 20) % (margin + 1)
    sizes = sizes.at[source_of].add(-shifted).at[taker].add(shifted)
    members = jnp.searchsorted(jnp.cumsum(sizes), jnp.arange(rows * top), side="right").astype(jnp.int32)
    grid = members.reshape(top, rows).T
    grid = grid[jax.random.permutation(jax.random.fold_in(own, 1), rows)]
    rotation = jax.random.randint(jax.random.fold_in(own, 2), (rows, 1), 0, top)
    return jnp.take_along_axis(grid, (jnp.arange(top)[None, :] + rotation) % top, axis=1)


def shares(amount, total, limit, slope, full):
    portions = [(1 << 20) // math.isqrt(grade ** slope) + 1 for grade in range(1, amount + 1)]
    largest = limit if full else min(limit, max(-(-total // amount), total * portions[0] // sum(portions)))
    least = 1 if total - largest >= amount - 1 else 0
    holding, rest = [largest] + [least] * (amount - 1), total - largest - least * (amount - 1)
    while rest > 0:
        candidates = [i for i in range(1, amount) if holding[i] < largest] or [i for i in range(1, amount) if holding[i] < limit]
        mass, remaining = sum([portions[i] for i in candidates]), rest
        for i in candidates:
            more = min(limit - holding[i], max(1, remaining * portions[i] // mass), rest)
            holding[i] = holding[i] + more
            rest = rest - more
    return np.array(holding)


def noise(rng, shape, deviation, bound, pieces=(), held_as=jnp.bfloat16):
    result = jax.random.normal(rng, shape, jnp.float32) * deviation
    if len(pieces) > 0:
        result = levels(rng, shape, pieces, -0.22, 0.18) * result
    return jnp.clip(result, min=-bound, max=bound).astype(held_as)


def heavy_noise(rng, shape, deviation, limit, pieces, heavy, kind=jnp.bfloat16):
    drawn = deviation * jax.random.normal(rng, shape, jnp.float32)
    if pieces:
        drawn = drawn * levels(rng, shape, pieces, -0.22, 0.18)
    return jnp.clip(with_spikes(drawn, jax.random.fold_in(rng, 3), *heavy), -limit, limit).astype(kind)


def setup_inputs(seed: int = 0) -> dict:
    streams_of = jax.random.split(jax.random.key(seed), 11)
    hidden = noise(streams_of[0], (TOKENS, D), 1.0, 6.0, ((0, 24), (1, 32)))
    norm_gain = jnp.clip(1.0 + 0.18 * jax.random.normal(streams_of[1], (D,), jnp.float32), 0.1, 1.9)
    routes_keys = jax.random.split(jax.random.fold_in(streams_of[2], 1), TOKENS // TOK_DEV)
    routes_turns = jax.random.permutation(jax.random.fold_in(streams_of[2], 3), TOKENS // TOK_DEV)
    routes = jax.vmap(lambda own, number: shared_out(jax.random.fold_in(streams_of[2], 2), own, number, TOK_DEV, EXPERTS, TOP_K, CAP, 2))(routes_keys, routes_turns).reshape((TOKENS, TOP_K))
    route_weights = jnp.clip(jnp.exp(math.log(1.0) - 2.3025851 * jax.random.uniform(streams_of[3], (TOKENS, TOP_K), jnp.float32) ** levels(streams_of[3], (TOKENS, TOP_K), ((0, 24),), -0.2, 0.2)), 0.1, 1.0)
    gate_weight = noise(streams_of[4], (EXPERTS, FF, D), D ** -0.5, 0.09375, ((0, 24), (1, 32)))
    up_weight = noise(streams_of[5], (EXPERTS, FF, D), D ** -0.5, 0.09375, ((0, 24), (1, 32)))
    down_weight = heavy_noise(streams_of[6], (EXPERTS, FF, D), FF ** -0.5, 0.375, ((0, 24), (1, 32)), (1, 2, 32, 2.75))
    shared_gate = noise(streams_of[7], (FFS, D), D ** -0.5, 0.09375, ((0, 32),))
    shared_up = noise(streams_of[8], (FFS, D), D ** -0.5, 0.09375, ((0, 32),))
    shared_down = heavy_noise(streams_of[9], (FFS, D), FFS ** -0.5, 0.375, ((0, 32),), (0, 1, 32, 2.75))
    return dict(hidden=hidden, norm_gain=norm_gain, routes=routes, route_weights=route_weights, gate_weight=gate_weight, up_weight=up_weight, down_weight=down_weight, shared_gate=shared_gate, shared_up=shared_up, shared_down=shared_down)


norm_eps = 1e-06

def norm_rows(hidden, norm_gain):
    values = hidden.astype(jnp.float32)
    inv_scale = lax.rsqrt(lax.optimization_barrier(jnp.mean(values * values, axis=-1, keepdims=True)) + norm_eps)
    return (values * inv_scale * norm_gain.astype(jnp.float32)).astype(jnp.bfloat16)

def slot_table(route_block):
    onehot = (route_block[:, :, None] == jnp.arange(EXPERTS, dtype=jnp.int32)[None, None, :]).astype(jnp.int32)
    used_mask = lax.optimization_barrier(jnp.sum(onehot, axis=1))
    before = jnp.cumsum(used_mask, axis=0) - used_mask
    slot_rank = lax.optimization_barrier(jnp.sum(onehot * before[:, None, :], axis=2))
    return (route_block * CAP + slot_rank).astype(jnp.int32)

def block_partials(inner_vals, down_w):
    row_count = inner_vals.shape[0]
    part_sums = jnp.einsum('rpf,pfd->rpd', inner_vals.reshape(row_count, N_TP, -1).astype(jnp.float32), down_w.reshape(N_TP, -1, D).astype(jnp.float32), precision=lax.Precision.HIGHEST)
    rounded = lax.optimization_barrier(part_sums.astype(jnp.bfloat16))
    return lax.optimization_barrier(jnp.sum(rounded.astype(jnp.float32), axis=1))

def expert_rows(row_block, gate_one, up_one, down_one):
    dims = (((1,), (1,)), ((), ()))
    gate_vals = lax.dot_general(row_block, gate_one, dims, preferred_element_type=jnp.float32)
    up_vals = lax.dot_general(row_block, up_one, dims, preferred_element_type=jnp.float32)
    inner_vals = (jax.nn.silu(gate_vals) * up_vals).astype(jnp.bfloat16)
    return block_partials(inner_vals, down_one)

def reference(hidden, norm_gain, routes, route_weights, gate_weight, up_weight, down_weight, shared_gate, shared_up, shared_down):
    normed = norm_rows(hidden, norm_gain)
    token_blocks = normed.reshape(N_EP, TOK_DEV, D)
    route_blocks = routes.reshape(N_EP, TOK_DEV, TOP_K)
    weight_blocks = route_weights.reshape(N_EP, TOK_DEV, TOP_K)
    slot_ids = jax.vmap(slot_table)(route_blocks)
    slot_range = jnp.arange(EXPERTS * CAP, dtype=jnp.int32)
    matches = slot_ids[:, :, :, None] == slot_range[None, None, None, :]
    select = lax.optimization_barrier(jnp.sum(matches.astype(jnp.float32), axis=2))
    combine = lax.optimization_barrier(jnp.sum(jnp.where(matches, weight_blocks[:, :, :, None], 0.0), axis=2))
    buffer = jnp.einsum('btr,btd->brd', select, token_blocks.astype(jnp.float32), precision=lax.Precision.HIGHEST).astype(jnp.bfloat16)
    buffer = buffer.reshape(N_EP, EXPERTS, CAP, D).transpose(1, 0, 2, 3).reshape(EXPERTS, N_EP * CAP, D)

    def one_expert(operands):
        row_block, gate_one, up_one, down_one = operands
        return expert_rows(row_block, gate_one, up_one, down_one).astype(jnp.bfloat16)
    expert_out = lax.map(one_expert, (buffer, gate_weight, up_weight, down_weight))
    expert_out = expert_out.reshape(EXPERTS, N_EP, CAP, D).transpose(1, 0, 2, 3).reshape(N_EP, EXPERTS * CAP, D)
    routed = jnp.einsum('btr,brd->btd', combine, expert_out.astype(jnp.float32), precision=lax.Precision.HIGHEST).reshape(TOKENS, D)
    shared = expert_rows(normed, shared_gate, shared_up, shared_down)
    return (routed + shared).astype(jnp.bfloat16)
```

```python
import functools

import jax
import jax.numpy as jnp
from jax import lax
from jax.experimental import pallas as pl
from jax.experimental.pallas import tpu as pltpu
from jax.sharding import Mesh, PartitionSpec as P

norm_eps = 1e-06
f32 = jnp.float32
bf16 = jnp.bfloat16

N_Z, N_C, N_Y, N_X = 12, 2, 8, 4
N_TP = N_Y * N_X
N_Q = 4
RANKS = 4
CAP = 3
TOK = 16
LOCAL = N_Q * RANKS
SLOTS = N_Z * LOCAL
ROWS = 40
ALL = ROWS + TOK
LANES = 128
HALF = 2048
UNITS = 32


def expert_of(j):
    return 2 * ((j // N_X) % 2) + j % 2


def iota(shape, dim):
    return lax.broadcasted_iota(jnp.int32, shape, dim)


def dot(a, b, dims, precision=None):
    return lax.dot_general(a, b, (dims, ((), ())), preferred_element_type=f32, precision=precision)


def pack_body(routes_ref, hidden_ref, out_ref):
    slot = iota((SLOTS, TOK), 0)
    named = jnp.zeros((SLOTS, TOK), f32)
    for k in range(4):
        named = named + jnp.where(routes_ref[k : k + 1, :] == slot // RANKS, 1.0, 0.0)
    earlier = jnp.where(iota((TOK, TOK), 0) < iota((TOK, TOK), 1), 1.0, 0.0)
    rank = dot(named.astype(bf16), earlier.astype(bf16), ((1,), (0,)))
    select = jnp.where(rank == (slot % RANKS).astype(f32), named, 0.0)
    out_ref[...] = dot(select.astype(bf16), hidden_ref[...], ((1,), (0,))).astype(bf16)


def combine_body(routes_ref, weights_ref, out_ref):
    slot = iota((TOK, SLOTS), 1)
    hits = [routes_ref[:, k : k + 1] == slot // RANKS for k in range(4)]
    named = sum(jnp.where(hit, 1.0, 0.0) for hit in hits)
    earlier = jnp.where(iota((TOK, TOK), 1) < iota((TOK, TOK), 0), 1.0, 0.0)
    rank = dot(earlier.astype(bf16), named.astype(bf16), ((1,), (0,)))
    here = rank == (slot % RANKS).astype(f32)
    total = sum(jnp.where(hits[k], weights_ref[:, k : k + 1], 0.0) for k in range(4))
    out_ref[...] = jnp.where(here, total, 0.0)


def slot_match(shape, slot_dim, row_dim):
    slot = iota(shape, slot_dim)
    row = iota(shape, row_dim)
    rank = slot % RANKS
    target = ((slot // RANKS) % N_Q) * ROWS + (slot // LOCAL) * CAP + rank
    return jnp.where((row == target) & (rank < CAP), 1.0, 0.0).astype(bf16)


def spread_body(arrived_ref, hidden_ref, out_ref):
    match = slot_match((N_Q * ROWS, SLOTS), 1, 0)
    rows = dot(match, arrived_ref[...], ((1,), (0,))).astype(bf16)
    own = hidden_ref[...]
    for j in range(N_TP):
        q = expert_of(j)
        out_ref[j, 0:ROWS, :] = rows[q * ROWS : (q + 1) * ROWS]
        out_ref[j, ROWS:ALL, :] = own


def weights_body(pos_ref, gate_ref, up_ref, down_ref, o0, o1, o2, o3, sems):
    copies = []
    for m, out in enumerate((o0, o1, o2, o3)):
        v = pos_ref[m]
        for w, ref in enumerate((gate_ref, up_ref, down_ref)):
            copy = pltpu.make_async_copy(
                ref.at[v % 2, :, pl.ds((v // 2) * HALF, HALF)], out.at[w], sems.at[m, w]
            )
            copy.start()
            copies.append(copy)
    for copy in copies:
        copy.wait()


def silu(v):
    return v / (1.0 + jnp.exp(-v))


def experts_body(core_ref, rows_ref, gain_ref, a0, a1, a2, a3, b0, b1, b2, b3, sg, su, sd, out_ref, normed):
    core = core_ref[0]
    squares = jnp.zeros((ALL, LANES), f32)
    for s in range(N_TP):
        v = rows_ref[s].astype(f32)
        squares = squares + v * v
    inv = lax.rsqrt(jnp.sum(squares, axis=1, keepdims=True) * (1.0 / (N_TP * LANES)) + norm_eps)
    for s in range(N_TP):
        normed[s] = (rows_ref[s].astype(f32) * inv * gain_ref[s]).astype(bf16)
    mine = (a0, a1, a2, a3)
    other = (b2, b3, b0, b1)
    nt = ((1,), (1,))

    def wide(first):
        return jnp.concatenate([normed[first + s] for s in range(N_TP // 2)], axis=1)

    x_mine = wide(core * (N_TP // 2))
    x_other = wide((1 - core) * (N_TP // 2))

    def project(w):
        w_mine = jnp.concatenate([ref[w] for ref in mine], axis=0)
        w_other = jnp.concatenate([ref[w] for ref in other], axis=0)
        return dot(x_mine[0:ROWS], w_mine, nt) + dot(x_other[0:ROWS], w_other, nt)

    inner = (silu(project(0)) * project(1)).astype(bf16)
    x_own = jnp.concatenate([normed[s, ROWS:ALL, :] for s in range(N_TP)], axis=1)
    shared = (silu(dot(x_own, sg[...], nt)) * dot(x_own, su[...], nt)).astype(bf16)
    nn = ((1,), (0,))
    for side, refs in ((core, mine), (1 - core, other)):
        w = jnp.concatenate([ref[2] for ref in refs], axis=0)
        part = dot(inner, w, nn).astype(bf16)
        for s in range(N_TP // 2):
            out_ref[side * (N_TP // 2) + s, 0:ROWS, :] = part[:, s * LANES : (s + 1) * LANES]
    part = dot(shared, sd[...], nn).astype(bf16)
    for s in range(N_TP):
        out_ref[s, ROWS:ALL, :] = part[:, s * LANES : (s + 1) * LANES]


def sum_body(parts_ref, out_ref, shared_ref):
    sums = []
    for q in range(N_Q):
        total = jnp.zeros((ROWS, LANES), f32)
        for s in range(N_TP):
            if expert_of(s) == q:
                total = total + parts_ref[s, 0:ROWS, :].astype(f32)
        sums.append(total.astype(bf16))
    match = slot_match((SLOTS, N_Q * ROWS), 0, 1)
    out_ref[...] = dot(match, jnp.concatenate(sums, axis=0), ((1,), (0,))).astype(bf16)
    shared = jnp.zeros((TOK, LANES), f32)
    for s in range(N_TP):
        shared = shared + parts_ref[s, ROWS:ALL, :].astype(f32)
    shared_ref[...] = shared


def final_body(combine_ref, returned_ref, shared_ref, out_ref):
    routed = dot(
        combine_ref[...], returned_ref[...].astype(f32), ((1,), (0,)), lax.Precision.HIGHEST
    )
    out_ref[...] = (routed + shared_ref[...]).astype(bf16)


VMEM = pl.BlockSpec(memory_space=pltpu.VMEM)
SMEM = pl.BlockSpec(memory_space=pltpu.SMEM)
ANY = pl.BlockSpec(memory_space=pl.ANY)


def call(body, name, ins, outs, *args, scratch=()):
    single = not isinstance(outs, list)
    shapes = [outs] if single else outs
    got = pl.pallas_call(
        body,
        name=name,
        in_specs=ins,
        out_specs=[VMEM if name != "weights" else ANY] * len(shapes),
        out_shape=shapes,
        scratch_shapes=list(scratch),
    )(*args)
    return got[0] if single else got


def shape(dims, dtype=bf16):
    return jax.ShapeDtypeStruct(dims, dtype)


def per_device(
    hidden,
    norm_gain,
    routes,
    route_weights,
    gate_weight,
    up_weight,
    down_weight,
    shared_gate,
    shared_up,
    shared_down,
):
    core, y, x = lax.axis_index("c"), lax.axis_index("y"), lax.axis_index("x")
    place = 2 * (y % 2) + x % 2
    packed = call(pack_body, "pack", [VMEM] * 2, shape((SLOTS, LANES)), routes.T, hidden)
    arrived = lax.all_to_all(packed.reshape(N_Z, LOCAL, LANES), "z", 0, 0, tiled=True)
    order = jnp.bitwise_xor(place, jnp.arange(4, dtype=jnp.int32))
    pieces = call(
        weights_body,
        "weights",
        [SMEM, ANY, ANY, ANY],
        [shape((3, UNITS, HALF))] * 4,
        order,
        gate_weight,
        up_weight,
        down_weight,
        scratch=[pltpu.SemaphoreType.DMA((4, 3))],
    )
    mine = []
    for m, piece in enumerate(pieces):
        pairs = []
        for c in range(N_C):
            for j in range(N_TP):
                sy, sx = j // N_X, j % N_X
                v = (2 * (sy % 2) + sx % 2) ^ m
                target = (v // 2) * N_TP + (sy - sy % 2 + c) * N_X + (sx - sx % 2 + v % 2)
                pairs.append((c * N_TP + j, target))
        mine.append(lax.ppermute(piece, ("c", "y", "x"), pairs))
    other = [lax.ppermute(piece, "c", [(0, 1), (1, 0)]) for piece in mine]
    combine = call(combine_body, "combine", [VMEM] * 2, shape((TOK, SLOTS), f32), routes, route_weights)
    spread = call(
        spread_body, "spread", [VMEM] * 2, shape((N_TP, ALL, LANES)), arrived.reshape(SLOTS, LANES), hidden
    )
    rows = lax.all_to_all(spread, ("y", "x"), 0, 0, tiled=True)
    parts = call(
        experts_body,
        "experts",
        [SMEM] + [VMEM] * 13,
        shape((N_TP, ALL, LANES)),
        core.reshape(1).astype(jnp.int32),
        rows,
        norm_gain.reshape(N_TP, 1, LANES),
        *mine,
        *other,
        shared_gate,
        shared_up,
        shared_down,
        scratch=[pltpu.VMEM((N_TP, ALL, LANES), bf16)],
    )
    parts = lax.all_to_all(parts, ("y", "x"), 0, 0, tiled=True)
    answers, shared_sum = call(
        sum_body, "sum", [VMEM], [shape((SLOTS, LANES)), shape((TOK, LANES), f32)], parts
    )
    returned = lax.all_to_all(answers.reshape(N_Z, LOCAL, LANES), "z", 0, 0, tiled=True)
    return call(
        final_body, "final", [VMEM] * 3, shape((TOK, LANES)), combine, returned.reshape(SLOTS, LANES), shared_sum
    )


def solution(mesh):
    fine = Mesh(mesh.devices.reshape(N_Z, N_C, N_Y, N_X), ("z", "c", "y", "x"))
    ep, tp = ("z", "c"), ("y", "x")
    in_specs = (
        P(ep, tp),
        P(),
        P(ep, None),
        P(ep, None),
        P(ep, tp, None),
        P(ep, tp, None),
        P(ep, tp, None),
        P(tp, None),
        P(tp, None),
        P(tp, None),
    )
    return jax.shard_map(
        per_device, mesh=fine, in_specs=in_specs, out_specs=P(ep, tp), check_vma=False
    )
```

```python
import jax
import jax.numpy as jnp
from jax import lax
from jax.experimental import pallas as pl
from jax.experimental.pallas import tpu as pltpu
from jax.sharding import Mesh, PartitionSpec as P

norm_eps = 1e-06
f32 = jnp.float32
bf16 = jnp.bfloat16

N_Z, N_C, N_Y, N_X = 12, 2, 8, 4
N_TP = N_Y * N_X
N_Q = 4
RANKS = 4
CAP = 3
TOK = 16
LOCAL = N_Q * RANKS
SLOTS = N_Z * LOCAL
ROWS = 40
ALL = ROWS + TOK
LANES = 128
HALF = 2048
UNITS = 32


def expert_of(j):
    return 2 * ((j // N_X) % 2) + j % 2


def iota(shape, dim):
    return lax.broadcasted_iota(jnp.int32, shape, dim)


def dot(a, b, dims, precision=None):
    return lax.dot_general(a, b, (dims, ((), ())), preferred_element_type=f32, precision=precision)


def pack_body(routes_ref, hidden_ref, out_ref):
    slot = iota((SLOTS, TOK), 0)
    named = jnp.zeros((SLOTS, TOK), f32)
    for k in range(4):
        named = named + jnp.where(routes_ref[k : k + 1, :] == slot // RANKS, 1.0, 0.0)
    earlier = jnp.where(iota((TOK, TOK), 0) < iota((TOK, TOK), 1), 1.0, 0.0)
    rank = dot(named.astype(bf16), earlier.astype(bf16), ((1,), (0,)))
    select = jnp.where(rank == (slot % RANKS).astype(f32), named, 0.0)
    out_ref[...] = dot(select.astype(bf16), hidden_ref[...], ((1,), (0,))).astype(bf16)


def combine_body(routes_ref, weights_ref, out_ref):
    slot = iota((TOK, SLOTS), 1)
    hits = [routes_ref[:, k : k + 1] == slot // RANKS for k in range(4)]
    named = sum(jnp.where(hit, 1.0, 0.0) for hit in hits)
    earlier = jnp.where(iota((TOK, TOK), 1) < iota((TOK, TOK), 0), 1.0, 0.0)
    rank = dot(earlier.astype(bf16), named.astype(bf16), ((1,), (0,)))
    here = rank == (slot % RANKS).astype(f32)
    total = sum(jnp.where(hits[k], weights_ref[:, k : k + 1], 0.0) for k in range(4))
    out_ref[...] = jnp.where(here, total, 0.0)


def slot_match(shape, slot_dim, row_dim):
    slot = iota(shape, slot_dim)
    row = iota(shape, row_dim)
    rank = slot % RANKS
    target = ((slot // RANKS) % N_Q) * ROWS + (slot // LOCAL) * CAP + rank
    return jnp.where((row == target) & (rank < CAP), 1.0, 0.0).astype(bf16)


def spread_body(arrived_ref, hidden_ref, out_ref):
    match = slot_match((N_Q * ROWS, SLOTS), 1, 0)
    rows = dot(match, arrived_ref[...], ((1,), (0,))).astype(bf16)
    own = hidden_ref[...]
    for j in range(N_TP):
        q = expert_of(j)
        out_ref[j, 0:ROWS, :] = rows[q * ROWS : (q + 1) * ROWS]
        out_ref[j, ROWS:ALL, :] = own


def weights_body(pos_ref, gate_ref, up_ref, down_ref, o0, o1, o2, o3, sems):
    copies = []
    for m, out in enumerate((o0, o1, o2, o3)):
        v = pos_ref[m]
        for w, ref in enumerate((gate_ref, up_ref, down_ref)):
            copy = pltpu.make_async_copy(
                ref.at[v % 2, :, pl.ds((v // 2) * HALF, HALF)], out.at[w], sems.at[m, w]
            )
            copy.start()
            copies.append(copy)
    for copy in copies:
        copy.wait()


def silu(v):
    return v / (1.0 + jnp.exp(-v))


def experts_body(core_ref, rows_ref, gain_ref, sg, su, sd, *refs):
    given, (out_ref, normed, held, sems) = refs[:8], refs[8:]
    copies = [pltpu.make_async_copy(given[i], held.at[i], sems.at[i]) for i in range(8)]
    for copy in copies:
        copy.start()
    core = core_ref[0]
    squares = jnp.zeros((ALL, LANES), f32)
    for s in range(N_TP):
        v = rows_ref[s].astype(f32)
        squares = squares + v * v
    inv = lax.rsqrt(jnp.sum(squares, axis=1, keepdims=True) * (1.0 / (N_TP * LANES)) + norm_eps)
    for s in range(N_TP):
        normed[s] = (rows_ref[s].astype(f32) * inv * gain_ref[s]).astype(bf16)
    mine = (0, 1, 2, 3)
    other = (6, 7, 4, 5)
    nt = ((1,), (1,))

    def wide(first):
        return jnp.concatenate([normed[first + s] for s in range(N_TP // 2)], axis=1)

    x_mine = wide(core * (N_TP // 2))
    x_other = wide((1 - core) * (N_TP // 2))

    for copy in copies:
        copy.wait()

    def project(w):
        w_mine = jnp.concatenate([held[i, w] for i in mine], axis=0)
        w_other = jnp.concatenate([held[i, w] for i in other], axis=0)
        return dot(x_mine[0:ROWS], w_mine, nt) + dot(x_other[0:ROWS], w_other, nt)

    inner = (silu(project(0)) * project(1)).astype(bf16)
    x_own = jnp.concatenate([normed[s, ROWS:ALL, :] for s in range(N_TP)], axis=1)
    shared = (silu(dot(x_own, sg[...], nt)) * dot(x_own, su[...], nt)).astype(bf16)
    nn = ((1,), (0,))
    for side, slots in ((core, mine), (1 - core, other)):
        w = jnp.concatenate([held[i, 2] for i in slots], axis=0)
        part = dot(inner, w, nn).astype(bf16)
        for s in range(N_TP // 2):
            out_ref[side * (N_TP // 2) + s, 0:ROWS, :] = part[:, s * LANES : (s + 1) * LANES]
    part = dot(shared, sd[...], nn).astype(bf16)
    for s in range(N_TP):
        out_ref[s, ROWS:ALL, :] = part[:, s * LANES : (s + 1) * LANES]


def sum_body(parts_ref, out_ref, shared_ref):
    sums = []
    for q in range(N_Q):
        total = jnp.zeros((ROWS, LANES), f32)
        for s in range(N_TP):
            if expert_of(s) == q:
                total = total + parts_ref[s, 0:ROWS, :].astype(f32)
        sums.append(total.astype(bf16))
    match = slot_match((SLOTS, N_Q * ROWS), 0, 1)
    out_ref[...] = dot(match, jnp.concatenate(sums, axis=0), ((1,), (0,))).astype(bf16)
    shared = jnp.zeros((TOK, LANES), f32)
    for s in range(N_TP):
        shared = shared + parts_ref[s, ROWS:ALL, :].astype(f32)
    shared_ref[...] = shared


def final_body(combine_ref, returned_ref, shared_ref, out_ref):
    routed = dot(
        combine_ref[...], returned_ref[...].astype(f32), ((1,), (0,)), lax.Precision.HIGHEST
    )
    out_ref[...] = (routed + shared_ref[...]).astype(bf16)


VMEM = pl.BlockSpec(memory_space=pltpu.VMEM)
SMEM = pl.BlockSpec(memory_space=pltpu.SMEM)
ANY = pl.BlockSpec(memory_space=pl.ANY)


def call(body, ins, outs, *args, scratch=(), limit=4):
    single = not isinstance(outs, list)
    shapes = [outs] if single else outs
    spaces = {id(VMEM): pltpu.VMEM, id(ANY): pltpu.HBM}
    args = [
        pltpu.with_memory_space_constraint(arg, spaces[id(spec)]) if id(spec) in spaces else arg
        for spec, arg in zip(ins, args, strict=True)
    ]
    got = pl.pallas_call(
        body,
        in_specs=ins,
        out_specs=[VMEM] * len(shapes),
        out_shape=shapes,
        scratch_shapes=list(scratch),
        compiler_params=pltpu.CompilerParams(vmem_limit_bytes=limit << 20),
    )(*args)
    return got[0] if single else got


def shape(dims, dtype=bf16):
    return pltpu.VMEM(dims, dtype)


def per_device(
    hidden,
    norm_gain,
    routes,
    route_weights,
    gate_weight,
    up_weight,
    down_weight,
    shared_gate,
    shared_up,
    shared_down,
):
    core, y, x = lax.axis_index("c"), lax.axis_index("y"), lax.axis_index("x")
    place = 2 * (y % 2) + x % 2
    packed = call(pack_body, [VMEM] * 2, shape((SLOTS, LANES)), routes.T, hidden)
    arrived = lax.all_to_all(packed.reshape(N_Z, LOCAL, LANES), "z", 0, 0, tiled=True)
    order = jnp.bitwise_xor(place, jnp.arange(4, dtype=jnp.int32))
    pieces = call(
        weights_body,
        [SMEM, ANY, ANY, ANY],
        [shape((3, UNITS, HALF))] * 4,
        order,
        gate_weight,
        up_weight,
        down_weight,
        scratch=[pltpu.SemaphoreType.DMA((4, 3))],
    )
    mine = []
    for m, piece in enumerate(pieces):
        pairs = []
        for c in range(N_C):
            for j in range(N_TP):
                sy, sx = j // N_X, j % N_X
                v = (2 * (sy % 2) + sx % 2) ^ m
                target = (v // 2) * N_TP + (sy - sy % 2 + c) * N_X + (sx - sx % 2 + v % 2)
                pairs.append((c * N_TP + j, target))
        mine.append(lax.ppermute(piece, ("c", "y", "x"), pairs))
    other = []
    for piece in mine:
        other.append(lax.ppermute(piece, "c", [(0, 1), (1, 0)]))
    combine = call(combine_body, [VMEM] * 2, shape((TOK, SLOTS), f32), routes, route_weights)
    spread = call(
        spread_body, [VMEM] * 2, shape((N_TP, ALL, LANES)), arrived.reshape(SLOTS, LANES), hidden
    )
    rows = lax.all_to_all(spread, ("y", "x"), 0, 0, tiled=True)
    parts = call(
        experts_body,
        [SMEM] + [VMEM] * 5 + [ANY] * 8,
        shape((N_TP, ALL, LANES)),
        core.reshape(1).astype(jnp.int32),
        rows,
        norm_gain.reshape(N_TP, 1, LANES),
        shared_gate,
        shared_up,
        shared_down,
        *mine,
        *other,
        scratch=[
            pltpu.VMEM((N_TP, ALL, LANES), bf16),
            pltpu.VMEM((8, 3, UNITS, HALF), bf16),
            pltpu.SemaphoreType.DMA((8,)),
        ],
        limit=24,
    )
    parts = lax.all_to_all(parts, ("y", "x"), 0, 0, tiled=True)
    answers, shared_sum = call(
        sum_body, [VMEM], [shape((SLOTS, LANES)), shape((TOK, LANES), f32)], parts
    )
    returned = lax.all_to_all(answers.reshape(N_Z, LOCAL, LANES), "z", 0, 0, tiled=True)
    return call(
        final_body, [VMEM] * 3, shape((TOK, LANES)), combine, returned.reshape(SLOTS, LANES), shared_sum
    )


def solution(mesh):
    fine = Mesh(mesh.devices.reshape(N_Z, N_C, N_Y, N_X), ("z", "c", "y", "x"))
    ep, tp = ("z", "c"), ("y", "x")
    in_specs = (
        P(ep, tp),
        P(),
        P(ep, None),
        P(ep, None),
        P(ep, tp, None),
        P(ep, tp, None),
        P(ep, tp, None),
        P(tp, None),
        P(tp, None),
        P(tp, None),
    )

    return jax.shard_map(
        per_device, mesh=fine, in_specs=in_specs, out_specs=P(ep, tp), check_vma=False
    )
```

```python
import jax
import jax.numpy as jnp
from jax import lax
from jax.experimental import pallas as pl
from jax.experimental.pallas import tpu as pltpu
from jax.sharding import Mesh, PartitionSpec as P

norm_eps = 1e-06
f32 = jnp.float32
bf16 = jnp.bfloat16

N_Z, N_C, N_Y, N_X = 12, 2, 8, 4
N_TP = N_Y * N_X
N_Q = 4
CAP = 3
TOK = 16
CAP = 3
TOK = 16
ROWS = N_Z * CAP
PADDED = 40
LANES = 128
HALF = 2048
UNITS = 32


def iota(shape, dim):
    return lax.broadcasted_iota(jnp.int32, shape, dim)


def dot(a, b, dims, precision=None):
    return lax.dot_general(a, b, (dims, ((), ())), preferred_element_type=f32, precision=precision)


def copies_body(hidden_ref, out_ref):
    for j in range(N_TP):
        out_ref[j] = hidden_ref[...]


def slot_of(shape, dim):
    row = iota(shape, dim)
    block = jnp.floor((row.astype(f32) + 0.5) * (1.0 / CAP)).astype(jnp.int32)
    return block, (row - CAP * block).astype(f32)


def tables_body(place_ref, across_ref, routes_ref, weights_ref, select_ref, combine_ref):
    place = place_ref[0]
    block, wanted = slot_of((PADDED, TOK), 0)
    named = jnp.zeros((PADDED, TOK), f32)
    for k in range(4):
        named = named + jnp.where(across_ref[k : k + 1, :] == N_Q * block + place, 1.0, 0.0)
    earlier = jnp.where(iota((TOK, TOK), 0) < iota((TOK, TOK), 1), 1.0, 0.0).astype(bf16)
    rank = dot(named.astype(bf16), earlier, ((1,), (0,)))
    select_ref[...] = jnp.where(rank == wanted, named, 0.0).astype(bf16)
    block, wanted = slot_of((TOK, PADDED), 1)
    named = jnp.zeros((TOK, PADDED), f32)
    total = jnp.zeros((TOK, PADDED), f32)
    for k in range(4):
        hit = routes_ref[:, k : k + 1] == N_Q * block + place
        named = named + jnp.where(hit, 1.0, 0.0)
        total = total + jnp.where(hit, weights_ref[:, k : k + 1], 0.0)
    earlier = jnp.where(iota((TOK, TOK), 1) < iota((TOK, TOK), 0), 1.0, 0.0).astype(bf16)
    rank = dot(earlier, named.astype(bf16), ((1,), (0,)))
    combine_ref[...] = jnp.where(rank == wanted, total, 0.0)


def norm_body(rows_ref, gain_ref, select_ref, own_ref, out_ref, flat):
    squares = jnp.zeros((TOK, LANES), f32)
    for s in range(N_TP):
        v = rows_ref[s].astype(f32)
        squares = squares + v * v
    inv = lax.rsqrt(jnp.sum(squares, axis=1, keepdims=True) * (1.0 / (N_TP * LANES)) + norm_eps)
    select = select_ref[...]
    for s in range(N_TP):
        piece = (rows_ref[s].astype(f32) * inv * gain_ref[s]).astype(bf16)
        own_ref[:, s * LANES : (s + 1) * LANES] = piece
        flat[pl.ds(s, ROWS, stride=N_TP), :] = dot(select, piece, ((1,), (0,)))[0:ROWS]
    out_ref[...] = flat[...].astype(bf16)


def weights_body(pos_ref, gate_ref, up_ref, down_ref, o0, o1, o2, o3, sems):
    copies = []
    for m, out in enumerate((o0, o1, o2, o3)):
        v = pos_ref[m]
        for w, ref in enumerate((gate_ref, up_ref, down_ref)):
            copy = pltpu.make_async_copy(
                ref.at[v % 2, :, pl.ds((v // 2) * HALF, HALF)], out.at[w], sems.at[m, w]
            )
            copy.start()
            copies.append(copy)
    for copy in copies:
        copy.wait()


def silu(v):
    return v / (1.0 + jnp.exp(-v))


def shared_body(own_ref, gate_ref, up_ref, down_ref, out_ref):
    own = own_ref[...]
    nt = ((1,), (1,))
    inner = (silu(dot(own, gate_ref[...], nt)) * dot(own, up_ref[...], nt)).astype(bf16)
    out_ref[...] = dot(inner, down_ref[...], ((1,), (0,)))


def experts_body(core_ref, rows_ref, *refs):
    given, (out_ref, flat, pieces, held, sems) = refs[:8], refs[8:]
    copies = [pltpu.make_async_copy(given[i], held.at[i], sems.at[i]) for i in range(8)]
    for copy in copies:
        copy.start()
    core = core_ref[0]
    flat[...] = rows_ref[...].astype(f32)
    for s in range(N_TP):
        pieces[s] = flat[pl.ds(s, ROWS, stride=N_TP), :].astype(bf16)

    def wide(first):
        return jnp.concatenate([pieces[first + s] for s in range(N_TP // 2)], axis=1)

    x_mine = wide(core * (N_TP // 2))
    x_other = wide((1 - core) * (N_TP // 2))
    mine = (0, 1, 2, 3)
    other = (6, 7, 4, 5)
    nt, nn = ((1,), (1,)), ((1,), (0,))
    for copy in copies:
        copy.wait()

    def project(w):
        w_mine = jnp.concatenate([held[i, w] for i in mine], axis=0)
        w_other = jnp.concatenate([held[i, w] for i in other], axis=0)
        return dot(x_mine, w_mine, nt) + dot(x_other, w_other, nt)

    inner = (silu(project(0)) * project(1)).astype(bf16)
    for side, slots in ((core, mine), (1 - core, other)):
        w = jnp.concatenate([held[i, 2] for i in slots], axis=0)
        part = dot(inner, w, nn)
        for s in range(N_TP // 2):
            flat[pl.ds(side * (N_TP // 2) + s, ROWS, stride=N_TP), :] = part[
                :, s * LANES : (s + 1) * LANES
            ]
    out_ref[...] = flat[...].astype(bf16)


def combine_body(rows_ref, combine_ref, shared_ref, out_ref, flat):
    flat[...] = rows_ref[...].astype(f32)
    combine = combine_ref[:, 0:ROWS]
    for s in range(N_TP):
        piece = flat[pl.ds(s, ROWS, stride=N_TP), :]
        total = dot(combine, piece, ((1,), (0,)), lax.Precision.HIGHEST)
        out_ref[s] = (total + shared_ref[:, s * LANES : (s + 1) * LANES]).astype(bf16)


def sum_body(parts_ref, out_ref):
    total = jnp.zeros((TOK, LANES), f32)
    for s in range(N_TP):
        total = total + parts_ref[s].astype(f32)
    out_ref[...] = total.astype(bf16)


VMEM = pl.BlockSpec(memory_space=pltpu.VMEM)
SMEM = pl.BlockSpec(memory_space=pltpu.SMEM)
ANY = pl.BlockSpec(memory_space=pl.ANY)


def call(body, ins, outs, *args, scratch=(), limit=4):
    single = not isinstance(outs, list)
    shapes = [outs] if single else outs
    spaces = {id(VMEM): pltpu.VMEM, id(ANY): pltpu.HBM}
    args = [
        pltpu.with_memory_space_constraint(arg, spaces[id(spec)]) if id(spec) in spaces else arg
        for spec, arg in zip(ins, args, strict=True)
    ]
    got = pl.pallas_call(
        body,
        in_specs=ins,
        out_specs=[VMEM] * len(shapes),
        out_shape=shapes,
        scratch_shapes=list(scratch),
        compiler_params=pltpu.CompilerParams(vmem_limit_bytes=limit << 20),
    )(*args)
    return got[0] if single else got


def shape(dims, dtype=bf16):
    return pltpu.VMEM(dims, dtype)


def per_device(
    hidden,
    norm_gain,
    routes,
    route_weights,
    gate_weight,
    up_weight,
    down_weight,
    shared_gate,
    shared_up,
    shared_down,
):
    core, y, x = lax.axis_index("c"), lax.axis_index("y"), lax.axis_index("x")
    place = 2 * (y % 2) + x % 2
    copies = call(copies_body, [VMEM], shape((N_TP, TOK, LANES)), hidden)
    tokens = lax.all_to_all(copies, ("y", "x"), 0, 0, tiled=True)
    select, combine = call(
        tables_body,
        [SMEM] + [VMEM] * 3,
        [shape((PADDED, TOK)), shape((TOK, PADDED), f32)],
        place.reshape(1).astype(jnp.int32),
        routes.T,
        routes,
        route_weights,
    )
    order = jnp.bitwise_xor(place, jnp.arange(4, dtype=jnp.int32))
    pieces = call(
        weights_body,
        [SMEM, ANY, ANY, ANY],
        [shape((3, UNITS, HALF))] * 4,
        order,
        gate_weight,
        up_weight,
        down_weight,
        scratch=[pltpu.SemaphoreType.DMA((4, 3))],
    )
    mine = []
    for m, piece in enumerate(pieces):
        pairs = []
        for c in range(N_C):
            for j in range(N_TP):
                sy, sx = j // N_X, j % N_X
                v = (2 * (sy % 2) + sx % 2) ^ m
                target = (v // 2) * N_TP + (sy - sy % 2 + c) * N_X + (sx - sx % 2 + v % 2)
                pairs.append((c * N_TP + j, target))
        mine.append(lax.ppermute(piece, ("c", "y", "x"), pairs))
    other = []
    for piece in mine:
        other.append(lax.ppermute(piece, "c", [(0, 1), (1, 0)]))
    flat = pltpu.VMEM((ROWS * N_TP, LANES), f32)
    own, packed = call(
        norm_body,
        [VMEM] * 3,
        [shape((TOK, N_TP * LANES)), shape((ROWS * N_TP, LANES))],
        tokens,
        norm_gain.reshape(N_TP, 1, LANES),
        select,
        scratch=[flat],
    )
    arrived = lax.all_to_all(packed.reshape(N_Z, CAP * N_TP, LANES), "z", 0, 0, tiled=True)
    shared = call(
        shared_body,
        [VMEM] * 4,
        shape((TOK, N_TP * LANES), f32),
        own,
        shared_gate,
        shared_up,
        shared_down,
    )
    parts = call(
        experts_body,
        [SMEM, VMEM] + [ANY] * 8,
        shape((ROWS * N_TP, LANES)),
        core.reshape(1).astype(jnp.int32),
        arrived.reshape(ROWS * N_TP, LANES),
        *mine,
        *other,
        scratch=[
            flat,
            pltpu.VMEM((N_TP, ROWS, LANES), bf16),
            pltpu.VMEM((8, 3, UNITS, HALF), bf16),
            pltpu.SemaphoreType.DMA((8,)),
        ],
        limit=24,
    )
    returned = lax.all_to_all(parts.reshape(N_Z, CAP * N_TP, LANES), "z", 0, 0, tiled=True)
    mixed = call(
        combine_body,
        [VMEM] * 3,
        shape((N_TP, TOK, LANES)),
        returned.reshape(ROWS * N_TP, LANES),
        combine,
        shared,
        scratch=[flat],
    )
    mixed = lax.all_to_all(mixed, ("y", "x"), 0, 0, tiled=True)
    return call(sum_body, [VMEM], shape((TOK, LANES)), mixed)


def solution(mesh):
    fine = Mesh(mesh.devices.reshape(N_Z, N_C, N_Y, N_X), ("z", "c", "y", "x"))
    ep, tp = ("z", "c"), ("y", "x")
    in_specs = (
        P(ep, tp),
        P(),
        P(ep, None),
        P(ep, None),
        P(ep, tp, None),
        P(ep, tp, None),
        P(ep, tp, None),
        P(tp, None),
        P(tp, None),
        P(tp, None),
    )

    return jax.shard_map(
        per_device, mesh=fine, in_specs=in_specs, out_specs=P(ep, tp), check_vma=False
    )
```

```python
import jax
import jax.numpy as jnp
from jax import lax
from jax.experimental import pallas as pl
from jax.experimental.pallas import tpu as pltpu
from jax.sharding import Mesh, PartitionSpec as P

norm_eps = 1e-06
f32 = jnp.float32
bf16 = jnp.bfloat16

N_Z, N_C, N_Y, N_X = 12, 2, 8, 4
N_TP = N_Y * N_X
N_Q = 4
CAP = 3
TOK = 16
CAP = 3
TOK = 16
ROWS = N_Z * CAP
PADDED = 40
LANES = 128
UNITS = 32


def iota(shape, dim):
    return lax.broadcasted_iota(jnp.int32, shape, dim)


def dot(a, b, dims, precision=None):
    return lax.dot_general(a, b, (dims, ((), ())), preferred_element_type=f32, precision=precision)


def copies_body(hidden_ref, out_ref):
    for j in range(N_TP):
        out_ref[j] = hidden_ref[...]


def slot_of(shape, dim):
    row = iota(shape, dim)
    block = jnp.floor((row.astype(f32) + 0.5) * (1.0 / CAP)).astype(jnp.int32)
    return block, (row - CAP * block).astype(f32)


def tables_body(place_ref, across_ref, routes_ref, weights_ref, select_ref, combine_ref):
    place = place_ref[0]
    block, wanted = slot_of((PADDED, TOK), 0)
    named = jnp.zeros((PADDED, TOK), f32)
    for k in range(4):
        named = named + jnp.where(across_ref[k : k + 1, :] == N_Q * block + place, 1.0, 0.0)
    earlier = jnp.where(iota((TOK, TOK), 0) < iota((TOK, TOK), 1), 1.0, 0.0).astype(bf16)
    rank = dot(named.astype(bf16), earlier, ((1,), (0,)))
    select_ref[...] = jnp.where(rank == wanted, named, 0.0).astype(bf16)
    block, wanted = slot_of((TOK, PADDED), 1)
    named = jnp.zeros((TOK, PADDED), f32)
    total = jnp.zeros((TOK, PADDED), f32)
    for k in range(4):
        hit = routes_ref[:, k : k + 1] == N_Q * block + place
        named = named + jnp.where(hit, 1.0, 0.0)
        total = total + jnp.where(hit, weights_ref[:, k : k + 1], 0.0)
    earlier = jnp.where(iota((TOK, TOK), 1) < iota((TOK, TOK), 0), 1.0, 0.0).astype(bf16)
    rank = dot(earlier, named.astype(bf16), ((1,), (0,)))
    combine_ref[...] = jnp.where(rank == wanted, total, 0.0)


def norm_body(rows_ref, gain_ref, select_ref, own_ref, out_ref, flat):
    squares = jnp.zeros((TOK, LANES), f32)
    for s in range(N_TP):
        v = rows_ref[s].astype(f32)
        squares = squares + v * v
    inv = lax.rsqrt(jnp.sum(squares, axis=1, keepdims=True) * (1.0 / (N_TP * LANES)) + norm_eps)
    select = select_ref[...]
    for s in range(N_TP):
        piece = (rows_ref[s].astype(f32) * inv * gain_ref[s]).astype(bf16)
        own_ref[:, s * LANES : (s + 1) * LANES] = piece
        flat[pl.ds(s, ROWS, stride=N_TP), :] = dot(select, piece, ((1,), (0,)))[0:ROWS]
    out_ref[...] = flat[...].astype(bf16)


def weights_body(first_ref, gate_ref, up_ref, down_ref, o0, o1, sems):
    copies = []
    for m, out in enumerate((o0, o1)):
        expert = (first_ref[0] + m) % 2
        for w, ref in enumerate((gate_ref, up_ref, down_ref)):
            copies.append(pltpu.make_async_copy(ref.at[expert], out.at[w], sems.at[m, w]))
            copies[-1].start()
    for copy in copies:
        copy.wait()


def silu(v):
    return v / (1.0 + jnp.exp(-v))


def shared_body(own_ref, gate_ref, up_ref, down_ref, out_ref):
    own = own_ref[...]
    nt = ((1,), (1,))
    inner = (silu(dot(own, gate_ref[...], nt)) * dot(own, up_ref[...], nt)).astype(bf16)
    out_ref[...] = dot(inner, down_ref[...], ((1,), (0,)))


def experts_body(rows_ref, g0, g1, g2, g3, out_ref, flat, held, sems):
    copies = [
        pltpu.make_async_copy(ref, held.at[:, pl.ds(i * UNITS, UNITS)], sems.at[i])
        for i, ref in enumerate((g0, g1, g2, g3))
    ]
    for copy in copies:
        copy.start()
    flat[...] = rows_ref[...].astype(f32)
    x = jnp.concatenate(
        [flat[pl.ds(s, ROWS, stride=N_TP), :].astype(bf16) for s in range(N_TP)], axis=1
    )
    for copy in copies:
        copy.wait()
    wide = held[0:2].reshape(2 * N_Q * UNITS, N_TP * LANES)
    both = dot(x, wide, ((1,), (1,)))
    inner = (silu(both[:, : N_Q * UNITS]) * both[:, N_Q * UNITS :]).astype(bf16)
    part = dot(inner, held[2], ((1,), (0,)))
    for s in range(N_TP):
        flat[pl.ds(s, ROWS, stride=N_TP), :] = part[:, s * LANES : (s + 1) * LANES]
    out_ref[...] = flat[...].astype(bf16)


def combine_body(rows_ref, combine_ref, shared_ref, out_ref, flat):
    flat[...] = rows_ref[...].astype(f32)
    combine = combine_ref[:, 0:ROWS]
    for s in range(N_TP):
        piece = flat[pl.ds(s, ROWS, stride=N_TP), :]
        total = dot(combine, piece, ((1,), (0,)), lax.Precision.HIGHEST)
        out_ref[s] = (total + shared_ref[:, s * LANES : (s + 1) * LANES]).astype(bf16)


def sum_body(parts_ref, out_ref):
    total = jnp.zeros((TOK, LANES), f32)
    for s in range(N_TP):
        total = total + parts_ref[s].astype(f32)
    out_ref[...] = total.astype(bf16)


VMEM = pl.BlockSpec(memory_space=pltpu.VMEM)
SMEM = pl.BlockSpec(memory_space=pltpu.SMEM)
ANY = pl.BlockSpec(memory_space=pl.ANY)
FREE = pl.BlockSpec(memory_space=pl.ANY)
LOAD = pl.BlockSpec(memory_space=pltpu.VMEM)


def call(body, ins, outs, *args, scratch=(), limit=4):
    single = not isinstance(outs, list)
    shapes = [outs] if single else outs
    spaces = {id(VMEM): pltpu.VMEM, id(ANY): pltpu.HBM}
    args = [
        pltpu.with_memory_space_constraint(arg, spaces[id(spec)]) if id(spec) in spaces else arg
        for spec, arg in zip(ins, args, strict=True)
    ]
    got = pl.pallas_call(
        body,
        in_specs=ins,
        out_specs=[VMEM] * len(shapes),
        out_shape=shapes,
        scratch_shapes=list(scratch),
        compiler_params=pltpu.CompilerParams(vmem_limit_bytes=limit << 20),
    )(*args)
    return got[0] if single else got


def shape(dims, dtype=bf16):
    return pltpu.VMEM(dims, dtype)


def per_device(
    hidden,
    norm_gain,
    routes,
    route_weights,
    gate_weight,
    up_weight,
    down_weight,
    shared_gate,
    shared_up,
    shared_down,
):
    y, x = lax.axis_index("y"), lax.axis_index("x")
    place = 2 * (y % 2) + x % 2
    copies = call(copies_body, [LOAD], shape((N_TP, TOK, LANES)), hidden)
    tokens = lax.all_to_all(copies, ("y", "x"), 0, 0, tiled=True)
    select, combine = call(
        tables_body,
        [SMEM] + [VMEM] * 3,
        [shape((PADDED, TOK)), shape((TOK, PADDED), f32)],
        place.reshape(1).astype(jnp.int32),
        routes.T,
        routes,
        route_weights,
    )
    pieces = call(
        weights_body,
        [SMEM, ANY, ANY, ANY],
        [shape((3, UNITS, N_TP * LANES))] * 2,
        (place % 2).reshape(1).astype(jnp.int32),
        gate_weight,
        up_weight,
        down_weight,
        scratch=[pltpu.SemaphoreType.DMA((2, 3))],
    )
    mine, other = [], []
    for m, piece in enumerate(pieces):
        pairs = []
        for c in range(N_C):
            for j in range(N_TP):
                sy, sx = j // N_X, j % N_X
                target = (sy % 2) * N_TP + (sy - sy % 2 + c) * N_X + (sx - sx % 2 + (sx + m) % 2)
                pairs.append((c * N_TP + j, target))
        mine.append(lax.ppermute(piece, ("c", "y", "x"), pairs))
        other.append(lax.ppermute(mine[-1], "c", [(0, 1), (1, 0)]))
    flat = pltpu.VMEM((ROWS * N_TP, LANES), f32)
    own, packed = call(
        norm_body,
        [VMEM] * 3,
        [shape((TOK, N_TP * LANES)), shape((ROWS * N_TP, LANES))],
        tokens,
        norm_gain.reshape(N_TP, 1, LANES),
        select,
        scratch=[flat],
    )
    arrived = lax.all_to_all(packed.reshape(N_Z, CAP * N_TP, LANES), "z", 0, 0, tiled=True)
    shared = call(
        shared_body,
        [VMEM] * 4,
        shape((TOK, N_TP * LANES), f32),
        own,
        shared_gate,
        shared_up,
        shared_down,
    )
    parts = call(
        experts_body,
        [VMEM] + [FREE] * 4,
        shape((ROWS * N_TP, LANES)),
        arrived.reshape(ROWS * N_TP, LANES),
        *mine,
        *other,
        scratch=[
            flat,
            pltpu.VMEM((3, N_Q * UNITS, N_TP * LANES), bf16),
            pltpu.SemaphoreType.DMA((4,)),
        ],
        limit=24,
    )
    returned = lax.all_to_all(parts.reshape(N_Z, CAP * N_TP, LANES), "z", 0, 0, tiled=True)
    mixed = call(
        combine_body,
        [VMEM] * 3,
        shape((N_TP, TOK, LANES)),
        returned.reshape(ROWS * N_TP, LANES),
        combine,
        shared,
        scratch=[flat],
    )
    mixed = lax.all_to_all(mixed, ("y", "x"), 0, 0, tiled=True)
    return call(sum_body, [VMEM], shape((TOK, LANES)), mixed)


def solution(mesh):
    fine = Mesh(mesh.devices.reshape(N_Z, N_C, N_Y, N_X), ("z", "c", "y", "x"))
    ep, tp = ("z", "c"), ("y", "x")
    in_specs = (
        P(ep, tp),
        P(),
        P(ep, None),
        P(ep, None),
        P(ep, tp, None),
        P(ep, tp, None),
        P(ep, tp, None),
        P(tp, None),
        P(tp, None),
        P(tp, None),
    )

    return jax.shard_map(
        per_device, mesh=fine, in_specs=in_specs, out_specs=P(ep, tp), check_vma=False
    )
```

```python
import jax
import jax.numpy as jnp
from jax import lax
from jax.experimental import pallas as pl
from jax.experimental.pallas import tpu as pltpu
from jax.sharding import Mesh, PartitionSpec as P

norm_eps = 1e-06
f32 = jnp.float32
bf16 = jnp.bfloat16

N_Z, N_C, N_Y, N_X = 12, 2, 8, 4
N_TP = N_Y * N_X
N_Q = 4
CAP = 3
TOK = 16
CAP = 3
TOK = 16
ROWS = N_Z * CAP
PADDED = 40
LANES = 128
UNITS = 32


def iota(shape, dim):
    return lax.broadcasted_iota(jnp.int32, shape, dim)


def dot(a, b, dims, precision=None):
    return lax.dot_general(a, b, (dims, ((), ())), preferred_element_type=f32, precision=precision)


def copies_body(hidden_ref, out_ref, own, sem):
    copy = pltpu.make_async_copy(hidden_ref, own, sem)
    copy.start()
    copy.wait()
    value = own[...]
    for j in range(N_TP):
        out_ref[j] = value


def slot_of(shape, dim):
    row = iota(shape, dim)
    block = jnp.floor((row.astype(f32) + 0.5) * (1.0 / CAP)).astype(jnp.int32)
    return block, (row - CAP * block).astype(f32)


def tables_body(place_ref, across_ref, routes_ref, weights_ref, gain_ref, select_ref, combine_ref, kept_ref):
    kept_ref[...] = gain_ref[...]
    place = place_ref[0]
    block, wanted = slot_of((PADDED, TOK), 0)
    named = jnp.zeros((PADDED, TOK), f32)
    for k in range(4):
        named = named + jnp.where(across_ref[k : k + 1, :] == N_Q * block + place, 1.0, 0.0)
    earlier = jnp.where(iota((TOK, TOK), 0) < iota((TOK, TOK), 1), 1.0, 0.0).astype(bf16)
    rank = dot(named.astype(bf16), earlier, ((1,), (0,)))
    select_ref[...] = jnp.where(rank == wanted, named, 0.0).astype(bf16)
    block, wanted = slot_of((TOK, PADDED), 1)
    named = jnp.zeros((TOK, PADDED), f32)
    total = jnp.zeros((TOK, PADDED), f32)
    for k in range(4):
        hit = routes_ref[:, k : k + 1] == N_Q * block + place
        named = named + jnp.where(hit, 1.0, 0.0)
        total = total + jnp.where(hit, weights_ref[:, k : k + 1], 0.0)
    earlier = jnp.where(iota((TOK, TOK), 1) < iota((TOK, TOK), 0), 1.0, 0.0).astype(bf16)
    rank = dot(earlier, named.astype(bf16), ((1,), (0,)))
    left = jnp.where(rank == wanted, total, 0.0)
    for n in range(3):
        term = left.astype(bf16)
        combine_ref[n * TOK : (n + 1) * TOK, :] = term
        left = left - term.astype(f32)


def norm_body(rows_ref, gain_ref, select_ref, own_ref, out_ref, flat, kept, sem):
    squares = jnp.zeros((TOK, LANES), f32)
    for s in range(N_TP):
        v = rows_ref[s].astype(f32)
        squares = squares + v * v
    inv = lax.rsqrt(jnp.sum(squares, axis=1, keepdims=True) * (1.0 / (N_TP * LANES)) + norm_eps)
    for s in range(N_TP):
        kept[:, s * LANES : (s + 1) * LANES] = (
            rows_ref[s].astype(f32) * inv * gain_ref[s : s + 1, :]
        ).astype(bf16)
    copy = pltpu.make_async_copy(kept, own_ref, sem)
    copy.start()
    select = select_ref[...]
    for s in range(N_TP):
        piece = kept[:, s * LANES : (s + 1) * LANES]
        flat[pl.ds(s, ROWS, stride=N_TP), :] = dot(select, piece, ((1,), (0,)))[0:ROWS]
    out_ref[...] = flat[...].astype(bf16)
    copy.wait()


def weights_body(first_ref, gate_ref, up_ref, down_ref, o0, o1, sems):
    copies = []
    for m, out in enumerate((o0, o1)):
        expert = (first_ref[0] + m) % 2
        for w, ref in enumerate((gate_ref, up_ref, down_ref)):
            copies.append(pltpu.make_async_copy(ref.at[expert], out.at[w], sems.at[m, w]))
            copies[-1].start()
    for copy in copies:
        copy.wait()


def silu(v):
    return v / (1.0 + jnp.exp(-v))


def shared_body(own_ref, gate_ref, up_ref, down_ref, out_ref):
    own = own_ref[...]
    nt = ((1,), (1,))
    inner = (silu(dot(own, gate_ref[...], nt)) * dot(own, up_ref[...], nt)).astype(bf16)
    out_ref[...] = dot(inner, down_ref[...], ((1,), (0,)))


def experts_body(rows_ref, g0, g1, g2, g3, out_ref, flat):
    given = (g0, g1, g2, g3)
    flat[...] = rows_ref[...].astype(f32)
    wide = 2 * LANES
    both = jnp.zeros((ROWS, 2 * N_Q * UNITS), f32)
    for n in range(N_TP // 2):
        x = jnp.concatenate(
            [flat[pl.ds(2 * n + h, ROWS, stride=N_TP), :].astype(bf16) for h in range(2)], axis=1
        )
        w = jnp.concatenate(
            [ref[p, :, n * wide : (n + 1) * wide] for p in range(2) for ref in given], axis=0
        )
        both = both + dot(x, w, ((1,), (1,)))
    inner = (silu(both[:, : N_Q * UNITS]) * both[:, N_Q * UNITS :]).astype(bf16)
    for n in range(N_TP // 2):
        w = jnp.concatenate([ref[2, :, n * wide : (n + 1) * wide] for ref in given], axis=0)
        part = dot(inner, w, ((1,), (0,)))
        for h in range(2):
            flat[pl.ds(2 * n + h, ROWS, stride=N_TP), :] = part[:, h * LANES : (h + 1) * LANES]
    out_ref[...] = flat[...].astype(bf16)


def combine_body(rows_ref, combine_ref, shared_ref, out_ref, flat):
    flat[...] = rows_ref[...].astype(f32)
    combine = combine_ref[:, 0:ROWS]
    for s in range(N_TP):
        piece = flat[pl.ds(s, ROWS, stride=N_TP), :].astype(bf16)
        terms = dot(combine, piece, ((1,), (0,)))
        total = terms[0:TOK] + terms[TOK : 2 * TOK] + terms[2 * TOK : 3 * TOK]
        out_ref[s] = (total + shared_ref[:, s * LANES : (s + 1) * LANES]).astype(bf16)


def sum_body(parts_ref, out_ref):
    total = jnp.zeros((TOK, LANES), f32)
    for s in range(N_TP):
        total = total + parts_ref[s].astype(f32)
    out_ref[...] = total.astype(bf16)


VMEM = pl.BlockSpec(memory_space=pltpu.VMEM)
SMEM = pl.BlockSpec(memory_space=pltpu.SMEM)
ANY = pl.BlockSpec(memory_space=pl.ANY)


def call(body, ins, outs, *args, scratch=(), limit=4, outspecs=None):
    single = not isinstance(outs, list)
    shapes = [outs] if single else outs
    spaces = {id(VMEM): pltpu.VMEM, id(ANY): pltpu.HBM}
    args = [
        pltpu.with_memory_space_constraint(arg, spaces[id(spec)]) if id(spec) in spaces else arg
        for spec, arg in zip(ins, args, strict=True)
    ]
    got = pl.pallas_call(
        body,
        in_specs=ins,
        out_specs=outspecs or [VMEM] * len(shapes),
        out_shape=shapes,
        scratch_shapes=list(scratch),
        compiler_params=pltpu.CompilerParams(vmem_limit_bytes=limit << 20),
    )(*args)
    return got[0] if single else got


def shape(dims, dtype=bf16):
    return pltpu.VMEM(dims, dtype)


def per_device(
    hidden,
    norm_gain,
    routes,
    route_weights,
    gate_weight,
    up_weight,
    down_weight,
    shared_gate,
    shared_up,
    shared_down,
):
    y, x = lax.axis_index("y"), lax.axis_index("x")
    place = 2 * (y % 2) + x % 2
    copies = call(
        copies_body,
        [ANY],
        shape((N_TP, TOK, LANES)),
        hidden,
        scratch=[pltpu.VMEM((TOK, LANES), bf16), pltpu.SemaphoreType.DMA],
    )
    tokens = lax.all_to_all(copies, ("y", "x"), 0, 0, tiled=True)
    select, combine, gain = call(
        tables_body,
        [SMEM] + [VMEM] * 4,
        [shape((PADDED, TOK)), shape((3 * TOK, PADDED)), shape((N_TP, LANES), f32)],
        place.reshape(1).astype(jnp.int32),
        routes.T,
        routes,
        route_weights,
        norm_gain.reshape(N_TP, LANES),
    )
    pieces = call(
        weights_body,
        [SMEM, ANY, ANY, ANY],
        [shape((3, UNITS, N_TP * LANES))] * 2,
        (place % 2).reshape(1).astype(jnp.int32),
        gate_weight,
        up_weight,
        down_weight,
        scratch=[pltpu.SemaphoreType.DMA((2, 3))],
    )
    mine, other = [], []
    for m, piece in enumerate(pieces):
        pairs = []
        for c in range(N_C):
            for j in range(N_TP):
                sy, sx = j // N_X, j % N_X
                target = (sy % 2) * N_TP + (sy - sy % 2 + c) * N_X + (sx - sx % 2 + (sx + m) % 2)
                pairs.append((c * N_TP + j, target))
        mine.append(lax.ppermute(piece, ("c", "y", "x"), pairs))
        other.append(lax.ppermute(mine[-1], "c", [(0, 1), (1, 0)]))
    flat = pltpu.VMEM((ROWS * N_TP, LANES), f32)
    own, packed = call(
        norm_body,
        [VMEM] * 3,
        [pltpu.HBM((TOK, N_TP * LANES), bf16), shape((ROWS * N_TP, LANES))],
        tokens,
        gain,
        select,
        scratch=[flat, pltpu.VMEM((TOK, N_TP * LANES), bf16), pltpu.SemaphoreType.DMA],
        outspecs=[ANY, VMEM],
    )
    arrived = lax.all_to_all(packed.reshape(N_Z, CAP * N_TP, LANES), "z", 0, 0, tiled=True)
    shared = call(
        shared_body,
        [VMEM] * 4,
        shape((TOK, N_TP * LANES), f32),
        own,
        shared_gate,
        shared_up,
        shared_down,
    )
    parts = call(
        experts_body,
        [VMEM] * 5,
        shape((ROWS * N_TP, LANES)),
        arrived.reshape(ROWS * N_TP, LANES),
        *mine,
        *other,
        scratch=[flat],
        limit=8,
    )
    returned = lax.all_to_all(parts.reshape(N_Z, CAP * N_TP, LANES), "z", 0, 0, tiled=True)
    mixed = call(
        combine_body,
        [VMEM] * 3,
        shape((N_TP, TOK, LANES)),
        returned.reshape(ROWS * N_TP, LANES),
        combine,
        shared,
        scratch=[flat],
    )
    mixed = lax.all_to_all(mixed, ("y", "x"), 0, 0, tiled=True)
    return call(sum_body, [VMEM], jax.ShapeDtypeStruct((TOK, LANES), bf16), mixed)


def solution(mesh):
    fine = Mesh(mesh.devices.reshape(N_Z, N_C, N_Y, N_X), ("z", "c", "y", "x"))
    ep, tp = ("z", "c"), ("y", "x")
    in_specs = (
        P(ep, tp),
        P(),
        P(ep, None),
        P(ep, None),
        P(ep, tp, None),
        P(ep, tp, None),
        P(ep, tp, None),
        P(tp, None),
        P(tp, None),
        P(tp, None),
    )

    return jax.shard_map(
        per_device, mesh=fine, in_specs=in_specs, out_specs=P(ep, tp), check_vma=False
    )
```

```python
import jax
import jax.numpy as jnp
from jax import lax
from jax.experimental import pallas as pl
from jax.experimental.pallas import tpu as pltpu
from jax.sharding import Mesh, PartitionSpec as P

norm_eps = 1e-06
f32 = jnp.float32
bf16 = jnp.bfloat16

N_Z, N_C, N_Y, N_X = 12, 2, 8, 4
N_TP = N_Y * N_X
N_Q = 4
CAP = 3
TOK = 16
CAP = 3
TOK = 16
ROWS = N_Z * CAP
PADDED = 40
LANES = 128
UNITS = 32


def iota(shape, dim):
    return lax.broadcasted_iota(jnp.int32, shape, dim)


def dot(a, b, dims, precision=None):
    return lax.dot_general(a, b, (dims, ((), ())), preferred_element_type=f32, precision=precision)


def copies_body(hidden_ref, out_ref, own, sem):
    copy = pltpu.make_async_copy(hidden_ref, own, sem)
    copy.start()
    copy.wait()
    value = own[...]
    for j in range(N_TP):
        out_ref[j] = value


def slot_of(shape, dim):
    row = iota(shape, dim)
    block = jnp.floor((row.astype(f32) + 0.5) * (1.0 / CAP)).astype(jnp.int32)
    return block, (row - CAP * block).astype(f32)


def tables_body(place_ref, across_ref, routes_ref, weights_ref, gain_ref, select_ref, combine_ref, kept_ref):
    kept_ref[...] = gain_ref[...]
    place = place_ref[0]
    block, wanted = slot_of((PADDED, TOK), 0)
    named = jnp.zeros((PADDED, TOK), f32)
    for k in range(4):
        named = named + jnp.where(across_ref[k : k + 1, :] == N_Q * block + place, 1.0, 0.0)
    earlier = jnp.where(iota((TOK, TOK), 0) < iota((TOK, TOK), 1), 1.0, 0.0).astype(bf16)
    rank = dot(named.astype(bf16), earlier, ((1,), (0,)))
    select_ref[...] = jnp.where(rank == wanted, named, 0.0).astype(bf16)
    block, wanted = slot_of((TOK, PADDED), 1)
    named = jnp.zeros((TOK, PADDED), f32)
    total = jnp.zeros((TOK, PADDED), f32)
    for k in range(4):
        hit = routes_ref[:, k : k + 1] == N_Q * block + place
        named = named + jnp.where(hit, 1.0, 0.0)
        total = total + jnp.where(hit, weights_ref[:, k : k + 1], 0.0)
    earlier = jnp.where(iota((TOK, TOK), 1) < iota((TOK, TOK), 0), 1.0, 0.0).astype(bf16)
    rank = dot(earlier, named.astype(bf16), ((1,), (0,)))
    left = jnp.where(rank == wanted, total, 0.0)
    for n in range(3):
        term = left.astype(bf16)
        combine_ref[n * TOK : (n + 1) * TOK, :] = term
        left = left - term.astype(f32)


def norm_body(rows_ref, gain_ref, select_ref, own_ref, out_ref, flat, kept, sem):
    squares = jnp.zeros((TOK, LANES), f32)
    for s in range(N_TP):
        v = rows_ref[s].astype(f32)
        squares = squares + v * v
    inv = lax.rsqrt(jnp.sum(squares, axis=1, keepdims=True) * (1.0 / (N_TP * LANES)) + norm_eps)
    for s in range(N_TP):
        kept[:, s * LANES : (s + 1) * LANES] = (
            rows_ref[s].astype(f32) * inv * gain_ref[s : s + 1, :]
        ).astype(bf16)
    copy = pltpu.make_async_copy(kept, own_ref, sem)
    copy.start()
    select = select_ref[...]
    for s in range(N_TP):
        piece = kept[:, s * LANES : (s + 1) * LANES]
        flat[pl.ds(s, ROWS, stride=N_TP), :] = dot(select, piece, ((1,), (0,)))[0:ROWS]
    out_ref[...] = flat[...].astype(bf16)
    copy.wait()


def weights_body(first_ref, gate_ref, up_ref, down_ref, o0, o1, sems):
    copies = []
    for m, out in enumerate((o0, o1)):
        expert = (first_ref[0] + 1 - m) % 2
        for w, ref in enumerate((gate_ref, up_ref, down_ref)):
            copies.append(pltpu.make_async_copy(ref.at[expert], out.at[w], sems.at[m, w]))
            copies[-1].start()
    for copy in copies:
        copy.wait()


def silu(v):
    return v / (1.0 + jnp.exp(-v))


def shared_body(own_ref, gate_ref, up_ref, down_ref, out_ref, own, gate, up, down, part, sems):
    pairs = ((own_ref, own), (gate_ref, gate), (up_ref, up), (down_ref, down))
    copies = [pltpu.make_async_copy(a, b, sems.at[i]) for i, (a, b) in enumerate(pairs)]
    for copy in copies:
        copy.start()
    for copy in copies:
        copy.wait()
    nt = ((1,), (1,))
    x = own[...]
    inner = (silu(dot(x, gate[...], nt)) * dot(x, up[...], nt)).astype(bf16)
    part[...] = dot(inner, down[...], ((1,), (0,)))
    copy = pltpu.make_async_copy(part, out_ref, sems.at[4])
    copy.start()
    copy.wait()


def experts_body(rows_ref, g0, g1, g2, g3, out_ref, flat):
    given = (g0, g1, g2, g3)
    flat[...] = rows_ref[...].astype(f32)
    wide = 2 * LANES
    both = jnp.zeros((ROWS, 2 * N_Q * UNITS), f32)
    for n in range(N_TP // 2):
        x = jnp.concatenate(
            [flat[pl.ds(2 * n + h, ROWS, stride=N_TP), :].astype(bf16) for h in range(2)], axis=1
        )
        w = jnp.concatenate(
            [ref[p, :, n * wide : (n + 1) * wide] for p in range(2) for ref in given], axis=0
        )
        both = both + dot(x, w, ((1,), (1,)))
    inner = (silu(both[:, : N_Q * UNITS]) * both[:, N_Q * UNITS :]).astype(bf16)
    for n in range(N_TP // 2):
        w = jnp.concatenate([ref[2, :, n * wide : (n + 1) * wide] for ref in given], axis=0)
        part = dot(inner, w, ((1,), (0,)))
        for h in range(2):
            flat[pl.ds(2 * n + h, ROWS, stride=N_TP), :] = part[:, h * LANES : (h + 1) * LANES]
    out_ref[...] = flat[...].astype(bf16)


def combine_body(rows_ref, combine_ref, shared_ref, out_ref, flat):
    flat[...] = rows_ref[...].astype(f32)
    combine = combine_ref[:, 0:ROWS]
    for s in range(N_TP):
        piece = flat[pl.ds(s, ROWS, stride=N_TP), :].astype(bf16)
        terms = dot(combine, piece, ((1,), (0,)))
        total = terms[0:TOK] + terms[TOK : 2 * TOK] + terms[2 * TOK : 3 * TOK]
        out_ref[s] = (total + shared_ref[:, s * LANES : (s + 1) * LANES]).astype(bf16)


def sum_body(parts_ref, out_ref):
    total = jnp.zeros((TOK, LANES), f32)
    for s in range(N_TP):
        total = total + parts_ref[s].astype(f32)
    out_ref[...] = total.astype(bf16)


VMEM = pl.BlockSpec(memory_space=pltpu.VMEM)
SMEM = pl.BlockSpec(memory_space=pltpu.SMEM)
ANY = pl.BlockSpec(memory_space=pl.ANY)


def call(body, ins, outs, *args, scratch=(), limit=4, outspecs=None):
    single = not isinstance(outs, list)
    shapes = [outs] if single else outs
    spaces = {id(VMEM): pltpu.VMEM, id(ANY): pltpu.HBM}
    args = [
        pltpu.with_memory_space_constraint(arg, spaces[id(spec)]) if id(spec) in spaces else arg
        for spec, arg in zip(ins, args, strict=True)
    ]
    got = pl.pallas_call(
        body,
        in_specs=ins,
        out_specs=outspecs or [VMEM] * len(shapes),
        out_shape=shapes,
        scratch_shapes=list(scratch),
        compiler_params=pltpu.CompilerParams(vmem_limit_bytes=limit << 20),
    )(*args)
    return got[0] if single else got


def shape(dims, dtype=bf16):
    return pltpu.VMEM(dims, dtype)


def per_device(
    hidden,
    norm_gain,
    routes,
    route_weights,
    gate_weight,
    up_weight,
    down_weight,
    shared_gate,
    shared_up,
    shared_down,
):
    y, x = lax.axis_index("y"), lax.axis_index("x")
    place = 2 * (y % 2) + x % 2
    copies = call(
        copies_body,
        [ANY],
        shape((N_TP, TOK, LANES)),
        hidden,
        scratch=[pltpu.VMEM((TOK, LANES), bf16), pltpu.SemaphoreType.DMA],
    )
    tokens = lax.all_to_all(copies, ("y", "x"), 0, 0, tiled=True)
    select, combine, gain = call(
        tables_body,
        [SMEM] + [VMEM] * 4,
        [shape((PADDED, TOK)), shape((3 * TOK, PADDED)), shape((N_TP, LANES), f32)],
        place.reshape(1).astype(jnp.int32),
        routes.T,
        routes,
        route_weights,
        norm_gain.reshape(N_TP, LANES),
    )
    pieces = call(
        weights_body,
        [SMEM, ANY, ANY, ANY],
        [shape((3, UNITS, N_TP * LANES))] * 2,
        (place % 2).reshape(1).astype(jnp.int32),
        gate_weight,
        up_weight,
        down_weight,
        scratch=[pltpu.SemaphoreType.DMA((2, 3))],
    )
    mine, other = [], []
    for m, piece in enumerate(pieces):
        pairs = []
        for c in range(N_C):
            for j in range(N_TP):
                sy, sx = j // N_X, j % N_X
                target = (sy % 2) * N_TP + (sy - sy % 2 + c) * N_X + (sx - sx % 2 + (sx + 1 - m) % 2)
                pairs.append((c * N_TP + j, target))
        mine.append(lax.ppermute(piece, ("c", "y", "x"), pairs))
        other.append(lax.ppermute(mine[-1], "c", [(0, 1), (1, 0)]))
    flat = pltpu.VMEM((ROWS * N_TP, LANES), f32)
    own, packed = call(
        norm_body,
        [VMEM] * 3,
        [pltpu.HBM((TOK, N_TP * LANES), bf16), shape((ROWS * N_TP, LANES))],
        tokens,
        gain,
        select,
        scratch=[flat, pltpu.VMEM((TOK, N_TP * LANES), bf16), pltpu.SemaphoreType.DMA],
        outspecs=[ANY, VMEM],
    )
    arrived = lax.all_to_all(packed.reshape(N_Z, CAP * N_TP, LANES), "z", 0, 0, tiled=True)
    shared = call(
        shared_body,
        [ANY] * 4,
        pltpu.HBM((TOK, N_TP * LANES), f32),
        own,
        shared_gate,
        shared_up,
        shared_down,
        scratch=[pltpu.VMEM((TOK, N_TP * LANES), bf16)]
        + [pltpu.VMEM((UNITS, N_TP * LANES), bf16)] * 3
        + [pltpu.VMEM((TOK, N_TP * LANES), f32), pltpu.SemaphoreType.DMA((5,))],
        outspecs=[ANY],
    )
    parts = call(
        experts_body,
        [VMEM] * 5,
        shape((ROWS * N_TP, LANES)),
        arrived.reshape(ROWS * N_TP, LANES),
        *mine,
        *other,
        scratch=[flat],
        limit=8,
    )
    returned = lax.all_to_all(parts.reshape(N_Z, CAP * N_TP, LANES), "z", 0, 0, tiled=True)
    mixed = call(
        combine_body,
        [VMEM] * 3,
        shape((N_TP, TOK, LANES)),
        returned.reshape(ROWS * N_TP, LANES),
        combine,
        shared,
        scratch=[flat],
    )
    mixed = lax.all_to_all(mixed, ("y", "x"), 0, 0, tiled=True)
    return call(sum_body, [VMEM], jax.ShapeDtypeStruct((TOK, LANES), bf16), mixed)


def solution(mesh):
    fine = Mesh(mesh.devices.reshape(N_Z, N_C, N_Y, N_X), ("z", "c", "y", "x"))
    ep, tp = ("z", "c"), ("y", "x")
    in_specs = (
        P(ep, tp),
        P(),
        P(ep, None),
        P(ep, None),
        P(ep, tp, None),
        P(ep, tp, None),
        P(ep, tp, None),
        P(tp, None),
        P(tp, None),
        P(tp, None),
    )

    return jax.shard_map(
        per_device, mesh=fine, in_specs=in_specs, out_specs=P(ep, tp), check_vma=False
    )
```

```python
import jax
import jax.numpy as jnp
from jax import lax
from jax.experimental import pallas as pl
from jax.experimental.pallas import tpu as pltpu
from jax.sharding import Mesh, PartitionSpec as P

norm_eps = 1e-06
f32 = jnp.float32
bf16 = jnp.bfloat16

N_Z, N_C, N_Y, N_X = 12, 2, 8, 4
N_TP = N_Y * N_X
N_Q = 4
CAP = 3
TOK = 16
CAP = 3
TOK = 16
ROWS = N_Z * CAP
PADDED = 40
LANES = 128
UNITS = 32


def iota(shape, dim):
    return lax.broadcasted_iota(jnp.int32, shape, dim)


def dot(a, b, dims, precision=None):
    return lax.dot_general(a, b, (dims, ((), ())), preferred_element_type=f32, precision=precision)


def copies_body(hidden_ref, out_ref, own, sem):
    copy = pltpu.make_async_copy(hidden_ref, own, sem)
    copy.start()
    copy.wait()
    value = own[...]
    for j in range(N_TP):
        out_ref[j] = value


def slot_of(shape, dim):
    row = iota(shape, dim)
    block = jnp.floor((row.astype(f32) + 0.5) * (1.0 / CAP)).astype(jnp.int32)
    return block, (row - CAP * block).astype(f32)


def tables_body(place_ref, across_ref, routes_ref, weights_ref, gain_ref, select_ref, combine_ref, kept_ref):
    kept_ref[...] = gain_ref[...]
    place = place_ref[0]
    block, wanted = slot_of((PADDED, TOK), 0)
    named = jnp.zeros((PADDED, TOK), f32)
    for k in range(4):
        named = named + jnp.where(across_ref[k : k + 1, :] == N_Q * block + place, 1.0, 0.0)
    earlier = jnp.where(iota((TOK, TOK), 0) < iota((TOK, TOK), 1), 1.0, 0.0).astype(bf16)
    rank = dot(named.astype(bf16), earlier, ((1,), (0,)))
    select_ref[...] = jnp.where(rank == wanted, named, 0.0).astype(bf16)
    block, wanted = slot_of((TOK, PADDED), 1)
    named = jnp.zeros((TOK, PADDED), f32)
    total = jnp.zeros((TOK, PADDED), f32)
    for k in range(4):
        hit = routes_ref[:, k : k + 1] == N_Q * block + place
        named = named + jnp.where(hit, 1.0, 0.0)
        total = total + jnp.where(hit, weights_ref[:, k : k + 1], 0.0)
    earlier = jnp.where(iota((TOK, TOK), 1) < iota((TOK, TOK), 0), 1.0, 0.0).astype(bf16)
    rank = dot(earlier, named.astype(bf16), ((1,), (0,)))
    left = jnp.where(rank == wanted, total, 0.0)
    for n in range(3):
        term = left.astype(bf16)
        combine_ref[n * TOK : (n + 1) * TOK, :] = term
        left = left - term.astype(f32)


def norm_body(rows_ref, gain_ref, select_ref, own_ref, out_ref, flat, kept, packed, sems):
    squares = [jnp.zeros((TOK, LANES), f32)] * 4
    for s in range(N_TP):
        v = rows_ref[s].astype(f32)
        squares[s % 4] = squares[s % 4] + v * v
    total = jnp.sum((squares[0] + squares[1]) + (squares[2] + squares[3]), axis=1, keepdims=True)
    inv = lax.rsqrt(total * (1.0 / (N_TP * LANES)) + norm_eps)
    for s in range(N_TP):
        kept[:, s * LANES : (s + 1) * LANES] = (
            rows_ref[s].astype(f32) * inv * gain_ref[s : s + 1, :]
        ).astype(bf16)
    own_copy = pltpu.make_async_copy(kept, own_ref, sems.at[0])
    own_copy.start()
    select = select_ref[...]
    for s in range(N_TP):
        piece = kept[:, s * LANES : (s + 1) * LANES]
        flat[pl.ds(s, ROWS, stride=N_TP), :] = dot(select, piece, ((1,), (0,)))[0:ROWS]
    packed[...] = flat[...].astype(bf16)
    out_copy = pltpu.make_async_copy(packed, out_ref, sems.at[1])
    out_copy.start()
    own_copy.wait()
    out_copy.wait()


def weights_body(first_ref, gate_ref, up_ref, down_ref, o0, o1, sems):
    copies = []
    for m, out in enumerate((o0, o1)):
        expert = (first_ref[0] + 1 - m) % 2
        for w, ref in enumerate((gate_ref, up_ref, down_ref)):
            copies.append(pltpu.make_async_copy(ref.at[expert], out.at[w], sems.at[m, w]))
            copies[-1].start()
    for copy in copies:
        copy.wait()


def silu(v):
    return v / (1.0 + jnp.exp(-v))


def shared_body(own_ref, gate_ref, up_ref, down_ref, out_ref, own, gate, up, down, part, sems):
    pairs = ((own_ref, own), (gate_ref, gate), (up_ref, up), (down_ref, down))
    copies = [pltpu.make_async_copy(a, b, sems.at[i]) for i, (a, b) in enumerate(pairs)]
    for copy in copies:
        copy.start()
    for copy in copies:
        copy.wait()
    nt = ((1,), (1,))
    x = own[...]
    inner = (silu(dot(x, gate[...], nt)) * dot(x, up[...], nt)).astype(bf16)
    part[...] = dot(inner, down[...], ((1,), (0,)))
    copy = pltpu.make_async_copy(part, out_ref, sems.at[4])
    copy.start()
    copy.wait()


def experts_body(rows_ref, g0, g1, g2, g3, out_ref, flat):
    given = (g0, g1, g2, g3)
    flat[...] = rows_ref[...].astype(f32)
    wide = 2 * LANES
    both = jnp.zeros((ROWS, 2 * N_Q * UNITS), f32)
    for n in range(N_TP // 2):
        x = jnp.concatenate(
            [flat[pl.ds(2 * n + h, ROWS, stride=N_TP), :].astype(bf16) for h in range(2)], axis=1
        )
        w = jnp.concatenate(
            [ref[p, :, n * wide : (n + 1) * wide] for p in range(2) for ref in given], axis=0
        )
        both = both + dot(x, w, ((1,), (1,)))
    inner = (silu(both[:, : N_Q * UNITS]) * both[:, N_Q * UNITS :]).astype(bf16)
    for n in range(N_TP // 2):
        w = jnp.concatenate([ref[2, :, n * wide : (n + 1) * wide] for ref in given], axis=0)
        part = dot(inner, w, ((1,), (0,)))
        for h in range(2):
            flat[pl.ds(2 * n + h, ROWS, stride=N_TP), :] = part[:, h * LANES : (h + 1) * LANES]
    out_ref[...] = flat[...].astype(bf16)


def combine_body(rows_ref, combine_ref, shared_ref, out_ref, flat):
    flat[...] = rows_ref[...].astype(f32)
    combine = combine_ref[:, 0:ROWS]
    for s in range(N_TP):
        piece = flat[pl.ds(s, ROWS, stride=N_TP), :].astype(bf16)
        terms = dot(combine, piece, ((1,), (0,)))
        total = terms[0:TOK] + terms[TOK : 2 * TOK] + terms[2 * TOK : 3 * TOK]
        out_ref[s] = (total + shared_ref[:, s * LANES : (s + 1) * LANES]).astype(bf16)


def sum_body(parts_ref, out_ref):
    total = jnp.zeros((TOK, LANES), f32)
    for s in range(N_TP):
        total = total + parts_ref[s].astype(f32)
    out_ref[...] = total.astype(bf16)


VMEM = pl.BlockSpec(memory_space=pltpu.VMEM)
SMEM = pl.BlockSpec(memory_space=pltpu.SMEM)
ANY = pl.BlockSpec(memory_space=pl.ANY)


def call(body, ins, outs, *args, scratch=(), limit=4, outspecs=None):
    single = not isinstance(outs, list)
    shapes = [outs] if single else outs
    spaces = {id(VMEM): pltpu.VMEM, id(ANY): pltpu.HBM}
    args = [
        pltpu.with_memory_space_constraint(arg, spaces[id(spec)]) if id(spec) in spaces else arg
        for spec, arg in zip(ins, args, strict=True)
    ]
    got = pl.pallas_call(
        body,
        in_specs=ins,
        out_specs=outspecs or [VMEM] * len(shapes),
        out_shape=shapes,
        scratch_shapes=list(scratch),
        compiler_params=pltpu.CompilerParams(vmem_limit_bytes=limit << 20),
    )(*args)
    return got[0] if single else got


def shape(dims, dtype=bf16):
    return pltpu.VMEM(dims, dtype)


def per_device(
    hidden,
    norm_gain,
    routes,
    route_weights,
    gate_weight,
    up_weight,
    down_weight,
    shared_gate,
    shared_up,
    shared_down,
):
    y, x = lax.axis_index("y"), lax.axis_index("x")
    place = 2 * (y % 2) + x % 2
    copies = call(
        copies_body,
        [ANY],
        shape((N_TP, TOK, LANES)),
        hidden,
        scratch=[pltpu.VMEM((TOK, LANES), bf16), pltpu.SemaphoreType.DMA],
    )
    tokens = lax.all_to_all(copies, ("y", "x"), 0, 0, tiled=True)
    select, combine, gain = call(
        tables_body,
        [SMEM] + [VMEM] * 4,
        [shape((PADDED, TOK)), shape((3 * TOK, PADDED)), shape((N_TP, LANES), f32)],
        place.reshape(1).astype(jnp.int32),
        routes.T,
        routes,
        route_weights,
        norm_gain.reshape(N_TP, LANES),
    )
    pieces = call(
        weights_body,
        [SMEM, ANY, ANY, ANY],
        [shape((3, UNITS, N_TP * LANES))] * 2,
        (place % 2).reshape(1).astype(jnp.int32),
        gate_weight,
        up_weight,
        down_weight,
        scratch=[pltpu.SemaphoreType.DMA((2, 3))],
    )
    mine, other = [], []
    for m, piece in enumerate(pieces):
        pairs = []
        for c in range(N_C):
            for j in range(N_TP):
                sy, sx = j // N_X, j % N_X
                target = (sy % 2) * N_TP + (sy - sy % 2 + c) * N_X + (sx - sx % 2 + (sx + 1 - m) % 2)
                pairs.append((c * N_TP + j, target))
        mine.append(lax.ppermute(piece, ("c", "y", "x"), pairs))
        other.append(lax.ppermute(mine[-1], "c", [(0, 1), (1, 0)]))
    flat = pltpu.VMEM((ROWS * N_TP, LANES), f32)
    own, packed = call(
        norm_body,
        [VMEM] * 3,
        [pltpu.HBM((TOK, N_TP * LANES), bf16), pltpu.HBM((ROWS * N_TP, LANES), bf16)],
        tokens,
        gain,
        select,
        scratch=[
            flat,
            pltpu.VMEM((TOK, N_TP * LANES), bf16),
            pltpu.VMEM((ROWS * N_TP, LANES), bf16),
            pltpu.SemaphoreType.DMA((2,)),
        ],
        outspecs=[ANY, ANY],
    )
    arrived = lax.all_to_all(packed.reshape(N_Z, CAP * N_TP, LANES), "z", 0, 0, tiled=True)
    shared = call(
        shared_body,
        [ANY] * 4,
        pltpu.HBM((TOK, N_TP * LANES), f32),
        own,
        shared_gate,
        shared_up,
        shared_down,
        scratch=[pltpu.VMEM((TOK, N_TP * LANES), bf16)]
        + [pltpu.VMEM((UNITS, N_TP * LANES), bf16)] * 3
        + [pltpu.VMEM((TOK, N_TP * LANES), f32), pltpu.SemaphoreType.DMA((5,))],
        outspecs=[ANY],
    )
    parts = call(
        experts_body,
        [VMEM] * 5,
        shape((ROWS * N_TP, LANES)),
        arrived.reshape(ROWS * N_TP, LANES),
        *mine,
        *other,
        scratch=[flat],
        limit=8,
    )
    returned = lax.all_to_all(parts.reshape(N_Z, CAP * N_TP, LANES), "z", 0, 0, tiled=True)
    mixed = call(
        combine_body,
        [VMEM] * 3,
        shape((N_TP, TOK, LANES)),
        returned.reshape(ROWS * N_TP, LANES),
        combine,
        shared,
        scratch=[flat],
    )
    mixed = lax.all_to_all(mixed, ("y", "x"), 0, 0, tiled=True)
    return call(sum_body, [VMEM], jax.ShapeDtypeStruct((TOK, LANES), bf16), mixed)


def solution(mesh):
    fine = Mesh(mesh.devices.reshape(N_Z, N_C, N_Y, N_X), ("z", "c", "y", "x"))
    ep, tp = ("z", "c"), ("y", "x")
    in_specs = (
        P(ep, tp),
        P(),
        P(ep, None),
        P(ep, None),
        P(ep, tp, None),
        P(ep, tp, None),
        P(ep, tp, None),
        P(tp, None),
        P(tp, None),
        P(tp, None),
    )

    return jax.shard_map(
        per_device, mesh=fine, in_specs=in_specs, out_specs=P(ep, tp), check_vma=False
    )
```

```python
import jax
import jax.numpy as jnp
from jax import lax
from jax.experimental import pallas as pl
from jax.experimental.pallas import tpu as pltpu
from jax.sharding import Mesh, PartitionSpec as P

norm_eps = 1e-06
f32 = jnp.float32
bf16 = jnp.bfloat16

N_Z, N_C, N_Y, N_X = 12, 2, 8, 4
N_TP = N_Y * N_X
N_Q = 4
CAP = 3
TOK = 16
CAP = 3
TOK = 16
ROWS = N_Z * CAP
PADDED = 40
LANES = 128
UNITS = 32


def iota(shape, dim):
    return lax.broadcasted_iota(jnp.int32, shape, dim)


def dot(a, b, dims, precision=None):
    return lax.dot_general(a, b, (dims, ((), ())), preferred_element_type=f32, precision=precision)


def first_body(bit_ref, hidden_ref, gate_ref, up_ref, down_ref, *refs):
    small, (copies_ref, o0, o1), kept, (own, wide, sems) = refs[:3], refs[3:6], refs[6:9], refs[9:]
    own_copy = pltpu.make_async_copy(hidden_ref, own, sems.at[0])
    own_copy.start()
    waits = []
    for i in range(3):
        waits.append(pltpu.make_async_copy(small[i], kept[i], sems.at[8 + i]))
        waits[-1].start()
    for m, out in enumerate((o0, o1)):
        expert = (bit_ref[0] + 1 - m) % 2
        for w, ref in enumerate((gate_ref, up_ref, down_ref)):
            waits.append(pltpu.make_async_copy(ref.at[expert], out.at[w], sems.at[1 + 3 * m + w]))
            waits[-1].start()
    own_copy.wait()
    value = own[...]
    for j in range(N_TP):
        wide[j] = value
    waits.append(pltpu.make_async_copy(wide, copies_ref, sems.at[7]))
    waits[-1].start()
    for copy in waits:
        copy.wait()


def slot_of(shape, dim):
    row = iota(shape, dim)
    block = jnp.floor((row.astype(f32) + 0.5) * (1.0 / CAP)).astype(jnp.int32)
    return block, (row - CAP * block).astype(f32)


def tables_body(place_ref, across_ref, weights_ref, select_ref, combine_ref):
    place = place_ref[0]
    block, wanted = slot_of((PADDED, TOK), 0)
    named = jnp.zeros((PADDED, TOK), f32)
    for k in range(4):
        named = named + jnp.where(across_ref[k : k + 1, :] == N_Q * block + place, 1.0, 0.0)
    row, column = iota((TOK, TOK), 0), iota((TOK, TOK), 1)
    earlier = jnp.where(row < column, 1.0, 0.0).astype(bf16)
    rank = dot(named.astype(bf16), earlier, ((1,), (0,)))
    select_ref[...] = jnp.where(rank == wanted, named, 0.0).astype(bf16)
    same = jnp.where(row == column, 1.0, 0.0)
    nt = ((1,), (1,))
    routes = dot(same, across_ref[...].astype(f32), nt, lax.Precision.HIGHEST)
    weights = dot(same, weights_ref[...], nt, lax.Precision.HIGHEST)
    block, wanted = slot_of((TOK, PADDED), 1)
    expert = (N_Q * block + place).astype(f32)
    named = jnp.zeros((TOK, PADDED), f32)
    total = jnp.zeros((TOK, PADDED), f32)
    for k in range(4):
        hit = routes[:, k : k + 1] == expert
        named = named + jnp.where(hit, 1.0, 0.0)
        total = total + jnp.where(hit, weights[:, k : k + 1], 0.0)
    earlier = jnp.where(column < row, 1.0, 0.0).astype(bf16)
    rank = dot(earlier, named.astype(bf16), ((1,), (0,)))
    left = jnp.where(rank == wanted, total, 0.0)
    for n in range(3):
        term = left.astype(bf16)
        combine_ref[n * TOK : (n + 1) * TOK, :] = term
        left = left - term.astype(f32)


def norm_body(rows_ref, gain_ref, select_ref, own_ref, out_ref, flat, kept, packed, sems):
    squares = [jnp.zeros((TOK, LANES), f32)] * 4
    for s in range(N_TP):
        v = rows_ref[s].astype(f32)
        squares[s % 4] = squares[s % 4] + v * v
    total = jnp.sum((squares[0] + squares[1]) + (squares[2] + squares[3]), axis=1, keepdims=True)
    inv = lax.rsqrt(total * (1.0 / (N_TP * LANES)) + norm_eps)
    for s in range(N_TP):
        kept[:, s * LANES : (s + 1) * LANES] = (
            rows_ref[s].astype(f32) * inv * gain_ref[s : s + 1, :]
        ).astype(bf16)
    own_copy = pltpu.make_async_copy(kept, own_ref, sems.at[0])
    own_copy.start()
    select = select_ref[...]
    for s in range(N_TP):
        piece = kept[:, s * LANES : (s + 1) * LANES]
        flat[pl.ds(s, ROWS, stride=N_TP), :] = dot(select, piece, ((1,), (0,)))[0:ROWS]
    packed[...] = flat[...].astype(bf16)
    out_copy = pltpu.make_async_copy(packed, out_ref, sems.at[1])
    out_copy.start()
    own_copy.wait()
    out_copy.wait()


def silu(v):
    return v / (1.0 + jnp.exp(-v))


def shared_body(own_ref, gate_ref, up_ref, down_ref, out_ref, own, gate, up, down, part, sems):
    pairs = ((own_ref, own), (gate_ref, gate), (up_ref, up), (down_ref, down))
    copies = [pltpu.make_async_copy(a, b, sems.at[i]) for i, (a, b) in enumerate(pairs)]
    for copy in copies:
        copy.start()
    for copy in copies:
        copy.wait()
    nt = ((1,), (1,))
    x = own[...]
    inner = (silu(dot(x, gate[...], nt)) * dot(x, up[...], nt)).astype(bf16)
    part[...] = dot(inner, down[...], ((1,), (0,)))
    copy = pltpu.make_async_copy(part, out_ref, sems.at[4])
    copy.start()
    copy.wait()


def experts_body(rows_ref, g0, g1, g2, g3, out_ref, flat):
    given = (g0, g1, g2, g3)
    flat[...] = rows_ref[...].astype(f32)
    wide = 2 * LANES
    both = jnp.zeros((ROWS, 2 * N_Q * UNITS), f32)
    for n in range(N_TP // 2):
        x = jnp.concatenate(
            [flat[pl.ds(2 * n + h, ROWS, stride=N_TP), :].astype(bf16) for h in range(2)], axis=1
        )
        w = jnp.concatenate(
            [ref[p, :, n * wide : (n + 1) * wide] for p in range(2) for ref in given], axis=0
        )
        both = both + dot(x, w, ((1,), (1,)))
    inner = (silu(both[:, : N_Q * UNITS]) * both[:, N_Q * UNITS :]).astype(bf16)
    for n in range(N_TP // 2):
        w = jnp.concatenate([ref[2, :, n * wide : (n + 1) * wide] for ref in given], axis=0)
        part = dot(inner, w, ((1,), (0,)))
        for h in range(2):
            flat[pl.ds(2 * n + h, ROWS, stride=N_TP), :] = part[:, h * LANES : (h + 1) * LANES]
    out_ref[...] = flat[...].astype(bf16)


def combine_body(rows_ref, combine_ref, shared_ref, out_ref, flat):
    flat[...] = rows_ref[...].astype(f32)
    combine = combine_ref[:, 0:ROWS]
    for s in range(N_TP):
        piece = flat[pl.ds(s, ROWS, stride=N_TP), :].astype(bf16)
        terms = dot(combine, piece, ((1,), (0,)))
        total = terms[0:TOK] + terms[TOK : 2 * TOK] + terms[2 * TOK : 3 * TOK]
        out_ref[s] = (total + shared_ref[:, s * LANES : (s + 1) * LANES]).astype(bf16)


def sum_body(parts_ref, out_ref):
    total = jnp.zeros((TOK, LANES), f32)
    for s in range(N_TP):
        total = total + parts_ref[s].astype(f32)
    out_ref[...] = total.astype(bf16)


VMEM = pl.BlockSpec(memory_space=pltpu.VMEM)
SMEM = pl.BlockSpec(memory_space=pltpu.SMEM)
ANY = pl.BlockSpec(memory_space=pl.ANY)


def call(body, ins, outs, *args, scratch=(), limit=4, outspecs=None):
    single = not isinstance(outs, list)
    shapes = [outs] if single else outs
    spaces = {id(VMEM): pltpu.VMEM, id(ANY): pltpu.HBM}
    args = [
        pltpu.with_memory_space_constraint(arg, spaces[id(spec)]) if id(spec) in spaces else arg
        for spec, arg in zip(ins, args, strict=True)
    ]
    got = pl.pallas_call(
        body,
        in_specs=ins,
        out_specs=outspecs or [VMEM] * len(shapes),
        out_shape=shapes,
        scratch_shapes=list(scratch),
        compiler_params=pltpu.CompilerParams(vmem_limit_bytes=limit << 20),
    )(*args)
    return got[0] if single else got


def shape(dims, dtype=bf16):
    return pltpu.VMEM(dims, dtype)


def per_device(
    hidden,
    norm_gain,
    routes,
    route_weights,
    gate_weight,
    up_weight,
    down_weight,
    shared_gate,
    shared_up,
    shared_down,
):
    y, x = lax.axis_index("y"), lax.axis_index("x")
    place = 2 * (y % 2) + x % 2
    piece = shape((3, UNITS, N_TP * LANES))
    copies, take0, take1, across, weights, gain = call(
        first_body,
        [SMEM] + [ANY] * 7,
        [
            pltpu.HBM((N_TP, TOK, LANES), bf16),
            piece,
            piece,
            shape(routes.shape[::-1], jnp.int32),
            shape(routes.shape[::-1], f32),
            shape((N_TP, LANES), f32),
        ],
        (x % 2).reshape(1).astype(jnp.int32),
        hidden,
        gate_weight,
        up_weight,
        down_weight,
        routes.T,
        route_weights.T,
        norm_gain.reshape(N_TP, LANES),
        scratch=[
            pltpu.VMEM((TOK, LANES), bf16),
            pltpu.VMEM((N_TP, TOK, LANES), bf16),
            pltpu.SemaphoreType.DMA((11,)),
        ],
        outspecs=[ANY] + [VMEM] * 5,
    )
    tokens = lax.all_to_all(copies, ("y", "x"), 0, 0, tiled=True)
    select, combine = call(
        tables_body,
        [SMEM] + [VMEM] * 2,
        [shape((PADDED, TOK)), shape((3 * TOK, PADDED))],
        place.reshape(1).astype(jnp.int32),
        across,
        weights,
    )
    mine, other = [], []
    for m, piece in enumerate((take0, take1)):
        pairs = []
        for c in range(N_C):
            for j in range(N_TP):
                sy, sx = j // N_X, j % N_X
                target = (sy % 2) * N_TP + (sy - sy % 2 + c) * N_X + (sx - sx % 2 + (sx + 1 - m) % 2)
                pairs.append((c * N_TP + j, target))
        mine.append(lax.ppermute(piece, ("c", "y", "x"), pairs))
        other.append(lax.ppermute(mine[-1], "c", [(0, 1), (1, 0)]))
    flat = pltpu.VMEM((ROWS * N_TP, LANES), f32)
    own, packed = call(
        norm_body,
        [VMEM] * 3,
        [pltpu.HBM((TOK, N_TP * LANES), bf16), pltpu.HBM((ROWS * N_TP, LANES), bf16)],
        tokens,
        gain,
        select,
        scratch=[
            flat,
            pltpu.VMEM((TOK, N_TP * LANES), bf16),
            pltpu.VMEM((ROWS * N_TP, LANES), bf16),
            pltpu.SemaphoreType.DMA((2,)),
        ],
        outspecs=[ANY, ANY],
    )
    arrived = lax.all_to_all(packed.reshape(N_Z, CAP * N_TP, LANES), "z", 0, 0, tiled=True)
    shared = call(
        shared_body,
        [ANY] * 4,
        pltpu.HBM((TOK, N_TP * LANES), f32),
        own,
        shared_gate,
        shared_up,
        shared_down,
        scratch=[pltpu.VMEM((TOK, N_TP * LANES), bf16)]
        + [pltpu.VMEM((UNITS, N_TP * LANES), bf16)] * 3
        + [pltpu.VMEM((TOK, N_TP * LANES), f32), pltpu.SemaphoreType.DMA((5,))],
        outspecs=[ANY],
    )
    parts = call(
        experts_body,
        [VMEM] * 5,
        shape((ROWS * N_TP, LANES)),
        arrived.reshape(ROWS * N_TP, LANES),
        *mine,
        *other,
        scratch=[flat],
        limit=8,
    )
    returned = lax.all_to_all(parts.reshape(N_Z, CAP * N_TP, LANES), "z", 0, 0, tiled=True)
    mixed = call(
        combine_body,
        [VMEM] * 3,
        shape((N_TP, TOK, LANES)),
        returned.reshape(ROWS * N_TP, LANES),
        combine,
        shared,
        scratch=[flat],
    )
    mixed = lax.all_to_all(mixed, ("y", "x"), 0, 0, tiled=True)
    return call(sum_body, [VMEM], jax.ShapeDtypeStruct((TOK, LANES), bf16), mixed)


def solution(mesh):
    fine = Mesh(mesh.devices.reshape(N_Z, N_C, N_Y, N_X), ("z", "c", "y", "x"))
    ep, tp = ("z", "c"), ("y", "x")
    in_specs = (
        P(ep, tp),
        P(),
        P(ep, None),
        P(ep, None),
        P(ep, tp, None),
        P(ep, tp, None),
        P(ep, tp, None),
        P(tp, None),
        P(tp, None),
        P(tp, None),
    )

    return jax.shard_map(
        per_device, mesh=fine, in_specs=in_specs, out_specs=P(ep, tp), check_vma=False
    )
```

```python
import jax
import jax.numpy as jnp
from jax import lax
from jax.experimental import pallas as pl
from jax.experimental.pallas import tpu as pltpu
from jax.sharding import Mesh, PartitionSpec as P

norm_eps = 1e-06
f32 = jnp.float32
bf16 = jnp.bfloat16

N_Z, N_C, N_Y, N_X = 12, 2, 8, 4
N_TP = N_Y * N_X
N_Q = 4
CAP = 3
TOK = 16
CAP = 3
TOK = 16
ROWS = N_Z * CAP
PADDED = 40
LANES = 128
UNITS = 32


def iota(shape, dim):
    return lax.broadcasted_iota(jnp.int32, shape, dim)


def dot(a, b, dims, precision=None):
    return lax.dot_general(a, b, (dims, ((), ())), preferred_element_type=f32, precision=precision)


def first_body(bit_ref, hidden_ref, gate_ref, up_ref, down_ref, *refs):
    small, (copies_ref, o0, o1), kept, (own, wide, sems) = refs[:3], refs[3:6], refs[6:9], refs[9:]
    own_copy = pltpu.make_async_copy(hidden_ref, own, sems.at[0])
    own_copy.start()
    waits = []
    for i in range(3):
        waits.append(pltpu.make_async_copy(small[i], kept[i], sems.at[8 + i]))
        waits[-1].start()
    for m, out in enumerate((o0, o1)):
        expert = (bit_ref[0] + 1 - m) % 2
        for w, ref in enumerate((gate_ref, up_ref, down_ref)):
            waits.append(pltpu.make_async_copy(ref.at[expert], out.at[w], sems.at[1 + 3 * m + w]))
            waits[-1].start()
    own_copy.wait()
    value = own[...]
    for j in range(N_TP):
        wide[j] = value
    waits.append(pltpu.make_async_copy(wide, copies_ref, sems.at[7]))
    waits[-1].start()
    for copy in waits:
        copy.wait()


def slot_of(shape, dim):
    row = iota(shape, dim)
    block = jnp.floor((row.astype(f32) + 0.5) * (1.0 / CAP)).astype(jnp.int32)
    return block, (row - CAP * block).astype(f32)


def tables_body(place_ref, across_ref, weights_ref, select_ref, combine_ref):
    place = place_ref[0]
    block, wanted = slot_of((PADDED, TOK), 0)
    named = jnp.zeros((PADDED, TOK), f32)
    for k in range(4):
        named = named + jnp.where(across_ref[k : k + 1, :] == N_Q * block + place, 1.0, 0.0)
    row, column = iota((TOK, TOK), 0), iota((TOK, TOK), 1)
    earlier = jnp.where(row < column, 1.0, 0.0).astype(bf16)
    rank = dot(named.astype(bf16), earlier, ((1,), (0,)))
    select_ref[...] = jnp.where(rank == wanted, named, 0.0).astype(bf16)
    same = jnp.where(row == column, 1.0, 0.0)
    nt = ((1,), (1,))
    routes = dot(same, across_ref[...].astype(f32), nt, lax.Precision.HIGHEST)
    weights = dot(same, weights_ref[...], nt, lax.Precision.HIGHEST)
    block, wanted = slot_of((TOK, PADDED), 1)
    expert = (N_Q * block + place).astype(f32)
    named = jnp.zeros((TOK, PADDED), f32)
    total = jnp.zeros((TOK, PADDED), f32)
    for k in range(4):
        hit = routes[:, k : k + 1] == expert
        named = named + jnp.where(hit, 1.0, 0.0)
        total = total + jnp.where(hit, weights[:, k : k + 1], 0.0)
    earlier = jnp.where(column < row, 1.0, 0.0).astype(bf16)
    rank = dot(earlier, named.astype(bf16), ((1,), (0,)))
    left = jnp.where(rank == wanted, total, 0.0)
    for n in range(3):
        term = left.astype(bf16)
        combine_ref[n * TOK : (n + 1) * TOK, :] = term
        left = left - term.astype(f32)


def norm_body(rows_ref, gain_ref, select_ref, own_ref, out_ref, flat, kept, packed, sems):
    squares = [jnp.zeros((TOK, LANES), f32)] * 4
    for s in range(N_TP):
        v = rows_ref[s].astype(f32)
        squares[s % 4] = squares[s % 4] + v * v
    total = jnp.sum((squares[0] + squares[1]) + (squares[2] + squares[3]), axis=1, keepdims=True)
    inv = lax.rsqrt(total * (1.0 / (N_TP * LANES)) + norm_eps)
    for s in range(N_TP):
        kept[:, s * LANES : (s + 1) * LANES] = (
            rows_ref[s].astype(f32) * inv * gain_ref[s : s + 1, :]
        ).astype(bf16)
    own_copy = pltpu.make_async_copy(kept, own_ref, sems.at[0])
    own_copy.start()
    select = select_ref[...]
    for s in range(N_TP):
        piece = kept[:, s * LANES : (s + 1) * LANES]
        flat[pl.ds(s, ROWS, stride=N_TP), :] = dot(select, piece, ((1,), (0,)))[0:ROWS]
    packed[...] = flat[...].astype(bf16)
    out_copy = pltpu.make_async_copy(packed, out_ref, sems.at[1])
    out_copy.start()
    own_copy.wait()
    out_copy.wait()


def silu(v):
    return v / (1.0 + jnp.exp(-v))


def shared_body(own_ref, gate_ref, up_ref, down_ref, out_ref, own, gate, up, down, part, sems):
    pairs = ((own_ref, own), (gate_ref, gate), (up_ref, up), (down_ref, down))
    copies = [pltpu.make_async_copy(a, b, sems.at[i]) for i, (a, b) in enumerate(pairs)]
    for copy in copies:
        copy.start()
    for copy in copies:
        copy.wait()
    nt = ((1,), (1,))
    x = own[...]
    inner = (silu(dot(x, gate[...], nt)) * dot(x, up[...], nt)).astype(bf16)
    part[...] = dot(inner, down[...], ((1,), (0,)))
    copy = pltpu.make_async_copy(part, out_ref, sems.at[4])
    copy.start()
    copy.wait()


def experts_body(rows_ref, g0, g1, g2, g3, out_ref, flat):
    given = (g0, g1, g2, g3)
    flat[...] = rows_ref[...].astype(f32)
    wide = 2 * LANES
    both = jnp.zeros((ROWS, 2 * N_Q * UNITS), f32)
    for n in range(N_TP // 2):
        x = jnp.concatenate(
            [flat[pl.ds(2 * n + h, ROWS, stride=N_TP), :].astype(bf16) for h in range(2)], axis=1
        )
        w = jnp.concatenate(
            [ref[p, :, n * wide : (n + 1) * wide] for p in range(2) for ref in given], axis=0
        )
        both = both + dot(x, w, ((1,), (1,)))
    inner = (silu(both[:, : N_Q * UNITS]) * both[:, N_Q * UNITS :]).astype(bf16)
    for n in range(N_TP // 2):
        w = jnp.concatenate([ref[2, :, n * wide : (n + 1) * wide] for ref in given], axis=0)
        part = dot(inner, w, ((1,), (0,)))
        for h in range(2):
            flat[pl.ds(2 * n + h, ROWS, stride=N_TP), :] = part[:, h * LANES : (h + 1) * LANES]
    out_ref[...] = flat[...].astype(bf16)


def combine_body(rows_ref, combine_ref, shared_ref, out_ref, flat):
    flat[...] = rows_ref[...].astype(f32)
    combine = combine_ref[:, 0:ROWS]
    for s in range(N_TP):
        piece = flat[pl.ds(s, ROWS, stride=N_TP), :].astype(bf16)
        terms = dot(combine, piece, ((1,), (0,)))
        total = terms[0:TOK] + terms[TOK : 2 * TOK] + terms[2 * TOK : 3 * TOK]
        out_ref[s] = (total + shared_ref[:, s * LANES : (s + 1) * LANES]).astype(bf16)


def sum_body(parts_ref, out_ref):
    total = jnp.zeros((TOK, LANES), f32)
    for s in range(N_TP):
        total = total + parts_ref[s].astype(f32)
    out_ref[...] = total.astype(bf16)


VMEM = pl.BlockSpec(memory_space=pltpu.VMEM)
SMEM = pl.BlockSpec(memory_space=pltpu.SMEM)
ANY = pl.BlockSpec(memory_space=pl.ANY)


def call(body, ins, outs, *args, scratch=(), limit=4, outspecs=None):
    single = not isinstance(outs, list)
    shapes = [outs] if single else outs
    spaces = {id(VMEM): pltpu.VMEM, id(ANY): pltpu.HBM}
    args = [
        pltpu.with_memory_space_constraint(arg, spaces[id(spec)]) if id(spec) in spaces else arg
        for spec, arg in zip(ins, args, strict=True)
    ]
    got = pl.pallas_call(
        body,
        in_specs=ins,
        out_specs=outspecs or [VMEM] * len(shapes),
        out_shape=shapes,
        scratch_shapes=list(scratch),
        compiler_params=pltpu.CompilerParams(vmem_limit_bytes=limit << 20),
    )(*args)
    return got[0] if single else got


def shape(dims, dtype=bf16):
    return pltpu.VMEM(dims, dtype)


def per_device(
    hidden,
    norm_gain,
    routes,
    route_weights,
    gate_weight,
    up_weight,
    down_weight,
    shared_gate,
    shared_up,
    shared_down,
):
    x = place = lax.axis_index("x")
    piece = shape((3, UNITS, N_TP * LANES))
    copies, take0, take1, across, weights, gain = call(
        first_body,
        [SMEM] + [ANY] * 7,
        [
            pltpu.HBM((N_TP, TOK, LANES), bf16),
            piece,
            piece,
            shape(routes.shape[::-1], jnp.int32),
            shape(routes.shape[::-1], f32),
            shape((N_TP, LANES), f32),
        ],
        (x % 2).reshape(1).astype(jnp.int32),
        hidden,
        gate_weight,
        up_weight,
        down_weight,
        routes.T,
        route_weights.T,
        norm_gain.reshape(N_TP, LANES),
        scratch=[
            pltpu.VMEM((TOK, LANES), bf16),
            pltpu.VMEM((N_TP, TOK, LANES), bf16),
            pltpu.SemaphoreType.DMA((11,)),
        ],
        outspecs=[ANY] + [VMEM] * 5,
    )
    tokens = lax.all_to_all(copies, ("y", "x"), 0, 0, tiled=True)
    select, combine = call(
        tables_body,
        [SMEM] + [VMEM] * 2,
        [shape((PADDED, TOK)), shape((3 * TOK, PADDED))],
        place.reshape(1).astype(jnp.int32),
        across,
        weights,
    )
    mine, other = [], []
    for m, piece in enumerate((take0, take1)):
        pairs = []
        for c in range(N_C):
            for j in range(N_TP):
                sy, sx = j // N_X, j % N_X
                target = (sx // 2) * N_TP + sy * N_X + 2 * c + (sx + 1 - m) % 2
                pairs.append((c * N_TP + j, target))
        mine.append(lax.ppermute(piece, ("c", "y", "x"), pairs))
        other.append(lax.ppermute(mine[-1], "c", [(0, 1), (1, 0)]))
    flat = pltpu.VMEM((ROWS * N_TP, LANES), f32)
    own, packed = call(
        norm_body,
        [VMEM] * 3,
        [pltpu.HBM((TOK, N_TP * LANES), bf16), pltpu.HBM((ROWS * N_TP, LANES), bf16)],
        tokens,
        gain,
        select,
        scratch=[
            flat,
            pltpu.VMEM((TOK, N_TP * LANES), bf16),
            pltpu.VMEM((ROWS * N_TP, LANES), bf16),
            pltpu.SemaphoreType.DMA((2,)),
        ],
        outspecs=[ANY, ANY],
    )
    arrived = lax.all_to_all(packed.reshape(N_Z, CAP * N_TP, LANES), "z", 0, 0, tiled=True)
    shared = call(
        shared_body,
        [ANY] * 4,
        pltpu.HBM((TOK, N_TP * LANES), f32),
        own,
        shared_gate,
        shared_up,
        shared_down,
        scratch=[pltpu.VMEM((TOK, N_TP * LANES), bf16)]
        + [pltpu.VMEM((UNITS, N_TP * LANES), bf16)] * 3
        + [pltpu.VMEM((TOK, N_TP * LANES), f32), pltpu.SemaphoreType.DMA((5,))],
        outspecs=[ANY],
    )
    parts = call(
        experts_body,
        [VMEM] * 5,
        shape((ROWS * N_TP, LANES)),
        arrived.reshape(ROWS * N_TP, LANES),
        *mine,
        *other,
        scratch=[flat],
        limit=8,
    )
    returned = lax.all_to_all(parts.reshape(N_Z, CAP * N_TP, LANES), "z", 0, 0, tiled=True)
    mixed = call(
        combine_body,
        [VMEM] * 3,
        shape((N_TP, TOK, LANES)),
        returned.reshape(ROWS * N_TP, LANES),
        combine,
        shared,
        scratch=[flat],
    )
    mixed = lax.all_to_all(mixed, ("y", "x"), 0, 0, tiled=True)
    return call(sum_body, [VMEM], jax.ShapeDtypeStruct((TOK, LANES), bf16), mixed)


def solution(mesh):
    fine = Mesh(mesh.devices.reshape(N_Z, N_C, N_Y, N_X), ("z", "c", "y", "x"))
    ep, tp = ("z", "c"), ("y", "x")
    in_specs = (
        P(ep, tp),
        P(),
        P(ep, None),
        P(ep, None),
        P(ep, tp, None),
        P(ep, tp, None),
        P(ep, tp, None),
        P(tp, None),
        P(tp, None),
        P(tp, None),
    )

    return jax.shard_map(
        per_device, mesh=fine, in_specs=in_specs, out_specs=P(ep, tp), check_vma=False
    )
```
